128 devices in a mesh: kv: 16 (over z, x), tp: 8 (over y, core).
Axes of the slice: x: 4, y: 4, z: 4, core: 2. Of those that a mesh axis runs over, the one named last changes fastest.
Arguments:
- tokens: bfloat16 [96, 4096], P(None, 'kv'), may hold values from -210 to 210
- norm_gain: float32 [4096], P('kv'), may hold values from 0.1 to 1.9
- w_query: bfloat16 [4096, 4096], P('kv', 'tp'), may hold values from -1 to 1
- w_key: bfloat16 [4096, 4096], P('kv', 'tp'), may hold values from -2 to 2
- w_value: bfloat16 [4096, 4096], P('kv', 'tp'), may hold values from -0.09375 to 0.09375
- w_output: bfloat16 [4096, 4096], P('tp', 'kv'), may hold values from -0.09375 to 0.09375
- cache_keys: bfloat16 [4, 8192, 4096], P(None, 'kv', 'tp'), may hold values from -820 to 820
- cache_values: bfloat16 [4, 8192, 4096], P(None, 'kv', 'tp'), may hold values from -6 to 6
- map_lambda: float32 [64], P('tp'), may hold values from 0.3 to 0.8
- out_gain: float32 [4096], P('tp'), may hold values from 0.1 to 1.9
- parents: int32 [4, 24], replicated, may hold values from -1 to 22, as said below
- lengths: int32 [4], replicated, may hold values from 4096 to 8144, as said below
- accepted: int32 [4], replicated, may hold values from 0 to 24
Outputs:
- mixed: bfloat16 [96, 4096], P(None, 'kv')
- new_keys: bfloat16 [4, 8192, 4096], P(None, 'kv', 'tp')
- new_values: bfloat16 [4, 8192, 4096], P(None, 'kv', 'tp')
The draws below stay inside these ranges and needn't reach their ends.
Inputs may be any that keep to these rules, and one draw needn't show every extreme that they name: parents[b, j] lies between -1 and j - 1. `lengths`: some sequence has exactly the largest value.
All inputs are finite; a program needn't handle non-finite values.
Results may differ from the reference program's by a relative error of at most 0.029.
Values may be sent and summed in bfloat16 or wider, within the bound.
No kernel may reach another device: no remote copies, remote signals or barrier semaphores. Data moves between devices by JAX's collectives and lax.ppermute only.
A program may use at most 128 MiB of HBM per device.

```python
import math
import jax
import jax.numpy as jnp
from jax import lax

D = 4096
HEADS = 64
HEAD = 64
QK = 32
SEQS = 4
POS_DEV = 512
PROP = 24
CACHE = 8192
ROWS = 96
N_KV = 16
N_TP = 8


def draw_tokens(key, part):
    column_rise = jnp.arange(D, dtype=jnp.float32) / (D - 1)
    shared_part = 0.8 ** 0.5
    own_part = 0.2 ** 0.5
    common = jax.random.normal(jax.random.fold_in(key, 11), (SEQS, 1, D), jnp.float32)
    own = jax.random.normal(key, (SEQS, PROP, D), jnp.float32)
    mixture = jnp.clip(shared_part * common + own_part * own, -6.0, 6.0).reshape(ROWS, D)
    values = mixture * jnp.exp(column_rise * 1.1)
    return values.astype(jnp.bfloat16)


def query_matrix(key):
    base = jnp.clip(jax.random.normal(jax.random.fold_in(key, 21), (D, HEADS * HEAD), jnp.float32), -6.0, 6.0)
    return base * D ** (-0.5)


def draw_w_query(key, part):
    return query_matrix(key).astype(jnp.bfloat16)


def draw_w_key(key, part):
    coupling = math.log(1.6 * CACHE) / math.sqrt(QK)
    noise = jnp.clip(jax.random.normal(jax.random.fold_in(key, 22), (D, HEADS * HEAD), jnp.float32), -6.0, 6.0)
    values = coupling * query_matrix(key) + noise * D ** (-0.5)
    return values.astype(jnp.bfloat16)


def draw_cache_keys(key, part):
    values = 1.7 * jnp.clip(jax.random.normal(key, (SEQS, CACHE, HEADS * HEAD), jnp.float32), -6.0, 6.0)
    return values.astype(jnp.bfloat16)


def draw_parents(key, part):
    limits = jnp.arange(PROP, dtype=jnp.int32)
    return jax.random.randint(key, (SEQS, PROP), -1, limits[None, :]).astype(jnp.int32)


def draw_lengths(key, part):
    drawn = jax.random.randint(key, (SEQS,), CACHE // 2, CACHE - 2 * PROP + 1)
    chosen = jax.random.randint(jax.random.fold_in(key, 1), (), 0, SEQS)
    return drawn.at[chosen].set(CACHE - 2 * PROP).astype(jnp.int32)


def with_ends(array, stream_key, least, high):
    longest = array.shape.index(max(array.shape))
    spots = []
    for shift in (0, 1):
        where = [jax.random.randint(jax.random.fold_in(stream_key, axis), (), 0, length) for axis, length in enumerate(array.shape)]
        where[longest] = (where[longest] + shift) % array.shape[longest]
        spots.append(tuple(where))
    return array.at[spots[0]].set(least).at[spots[1]].set(high)


def block_levels(own_key, extent, shards, smallest, largest):
    factor_of = 1.0
    for position, shards_of in shards:
        heights = jax.random.uniform(jax.random.fold_in(jax.random.fold_in(own_key, 6), position), (shards_of,), jnp.float32, smallest / len(shards), largest / len(shards))
        factor_of = factor_of * jnp.repeat(jnp.exp(heights), extent[position] // shards_of).reshape((-1,) + (1,) * (len(extent) - 1 - position))
    return factor_of


def bell_draw(own_key, shape, scale, reach, split=(), kind=jnp.bfloat16):
    values = scale * jax.random.normal(own_key, shape, jnp.float32)
    if split:
        values = values * block_levels(own_key, shape, split, -0.22, 0.18)
    return jnp.clip(values, -reach, reach).astype(kind)


def setup_inputs(seed: int = 0) -> dict:
    keys = jax.random.split(jax.random.key(seed), 14)
    tokens = draw_tokens(jax.random.fold_in(keys[13], 71), 0)
    norm_gain = jnp.clip(1.0 + 0.18 * jax.random.normal(keys[1], (D,), jnp.float32), 0.1, 1.9)
    w_query = draw_w_query(jax.random.fold_in(keys[13], 71), 0)
    w_key = draw_w_key(jax.random.fold_in(keys[13], 71), 0)
    w_value = bell_draw(keys[4], (D, HEADS * HEAD), D ** -0.5, 0.09375, ((0, 16), (1, 8)))
    w_output = bell_draw(keys[5], (HEADS * HEAD, D), (HEADS * HEAD) ** -0.5, 0.09375, ((0, 8), (1, 16)))
    cache_keys = draw_cache_keys(jax.random.fold_in(keys[13], 71), 0)
    cache_values = bell_draw(keys[7], (SEQS, CACHE, HEADS * HEAD), 1.0, 6.0, ((1, 16), (2, 8)))
    map_lambda = jnp.clip(0.3 + 0.5 * jax.random.uniform(keys[8], (HEADS,), jnp.float32) ** block_levels(keys[8], (HEADS,), ((0, 8),), -0.2, 0.2), 0.3, 0.8)
    out_gain = jnp.clip(1.0 + 0.18 * jax.random.normal(keys[9], (HEADS * HEAD,), jnp.float32), 0.1, 1.9)
    parents = draw_parents(jax.random.fold_in(keys[13], 71), 0)
    lengths = draw_lengths(jax.random.fold_in(keys[13], 71), 0)
    accepted = with_ends(jax.random.randint(keys[12], (SEQS,), 0, PROP + 1), jax.random.fold_in(keys[12], 1), 0, PROP).astype(jnp.int32)
    return dict(tokens=tokens, norm_gain=norm_gain, w_query=w_query, w_key=w_key, w_value=w_value, w_output=w_output, cache_keys=cache_keys, cache_values=cache_values, map_lambda=map_lambda, out_gain=out_gain, parents=parents, lengths=lengths, accepted=accepted)


epsilon = 1e-05
masked_low = -1e+30

def ancestry(parents):
    count = parents.shape[1]
    places = jnp.arange(count, dtype=jnp.int32)
    parent_links = (parents[:, :, None] == places[None, None, :]).astype(jnp.float32)
    identity = jnp.eye(count, dtype=jnp.float32)[None]

    def extend(turn_index, reached):
        return jnp.minimum(1.0, identity + jnp.einsum('bji,bik->bjk', parent_links, reached))
    reached = lax.fori_loop(0, count, extend, jnp.broadcast_to(identity, parent_links.shape))
    return reached > 0.5

def reference(tokens, norm_gain, w_query, w_key, w_value, w_output, cache_keys, cache_values, map_lambda, out_gain, parents, lengths, accepted):
    f32 = jnp.float32
    bf16 = jnp.bfloat16
    tokens_wide = tokens.astype(f32)
    norm_factor = lax.rsqrt(lax.optimization_barrier(jnp.mean(tokens_wide * tokens_wide, axis=1, keepdims=True)) + epsilon)
    gained = (tokens_wide * norm_gain).astype(bf16)

    def projection(weight_matrix):
        return (jnp.dot(gained, weight_matrix, preferred_element_type=f32) * norm_factor).astype(bf16)
    queries = projection(w_query)
    keys_flat = projection(w_key)
    values_flat = projection(w_value)
    query_heads = queries.astype(f32).reshape(SEQS, PROP, HEADS, 2, QK)
    key_heads = keys_flat.astype(f32).reshape(SEQS, PROP, HEADS, 2, QK)
    value_heads = values_flat.reshape(SEQS, PROP, HEADS, HEAD)
    start = lengths + accepted
    score_scale = QK ** (-0.5)

    def cache_block(block_index):
        begin = (block_index * POS_DEV).astype(jnp.int32)
        block_keys = lax.dynamic_slice_in_dim(cache_keys, begin, POS_DEV, 1).astype(f32)
        block_keys = block_keys.reshape(SEQS, POS_DEV, HEADS, 2, QK)
        block_vals = lax.dynamic_slice_in_dim(cache_values, begin, POS_DEV, 1).astype(f32)
        block_vals = block_vals.reshape(SEQS, POS_DEV, HEADS, HEAD)
        positions = begin + jnp.arange(POS_DEV, dtype=jnp.int32)
        visible = (positions[None, :] < start[:, None])[:, None, None, None, :]
        scores = jnp.einsum('bqhmd,bkhmd->bmhqk', query_heads, block_keys) * score_scale
        block_max = lax.optimization_barrier(jnp.max(jnp.where(visible, scores, masked_low), axis=-1))
        block_weight = jnp.where(visible, jnp.exp(scores - block_max[..., None]), 0.0)
        block_total = lax.optimization_barrier(jnp.sum(block_weight, axis=-1))
        rounded = block_weight.astype(bf16).astype(f32)
        block_values = jnp.einsum('bmhqk,bkhd->bmhqd', rounded, block_vals).astype(bf16)
        return (block_max, block_total, block_values)
    maxima, totals, values = lax.map(cache_block, jnp.arange(N_KV, dtype=jnp.int32))
    cache_max = lax.optimization_barrier(jnp.max(maxima, axis=0))
    factors = jnp.exp(maxima - cache_max[None])
    cache_total = lax.optimization_barrier(jnp.sum(totals * factors, axis=0))
    cache_sum = lax.optimization_barrier(jnp.sum(values.astype(f32) * factors[..., None], axis=0))
    lineage = ancestry(parents)[:, None, None, :, :]
    self_scores = jnp.einsum('bqhmd,bjhmd->bmhqj', query_heads, key_heads) * score_scale
    self_max = lax.optimization_barrier(jnp.max(jnp.where(lineage, self_scores, masked_low), axis=-1))
    top = jnp.maximum(cache_max, self_max)
    self_weight = jnp.where(lineage, jnp.exp(self_scores - top[..., None]), 0.0)
    carried = jnp.exp(cache_max - top)
    denominator = cache_total * carried + lax.optimization_barrier(jnp.sum(self_weight, axis=-1))
    self_values = jnp.einsum('bmhqj,bjhd->bmhqd', self_weight.astype(bf16).astype(f32), value_heads.astype(f32))
    attended = (cache_sum * carried[..., None] + self_values) / denominator[..., None]
    difference = attended[:, 0] - map_lambda[None, :, None, None] * attended[:, 1]
    gains = out_gain.reshape(HEADS, HEAD)[None, :, None, :]
    normed = difference * lax.rsqrt(lax.optimization_barrier(jnp.mean(difference * difference, axis=-1, keepdims=True)) + epsilon) * gains
    normed = jnp.transpose(normed, (0, 2, 1, 3)).reshape(ROWS, HEADS * HEAD).astype(bf16)
    group = HEADS // N_TP
    pieces = normed.reshape(ROWS, N_TP, group * HEAD).astype(f32)
    weight_groups = w_output.reshape(N_TP, group * HEAD, D).astype(f32)
    partials = jnp.einsum('rgc,gcd->grd', pieces, weight_groups).astype(bf16)
    partials = lax.optimization_barrier(partials).astype(f32)
    mixed = lax.optimization_barrier(jnp.sum(partials, axis=0)).astype(bf16)

    def place(cache_row, new_rows, begin):
        return lax.dynamic_update_slice(cache_row, new_rows, (begin, jnp.int32(0)))
    new_keys = jax.vmap(place)(cache_keys, keys_flat.reshape(SEQS, PROP, HEADS * HEAD), start)
    new_values = jax.vmap(place)(cache_values, values_flat.reshape(SEQS, PROP, HEADS * HEAD), start)
    return (mixed, new_keys, new_values)
```

```python
import functools

import jax
import jax.numpy as jnp
from jax import lax
from jax.experimental import pallas as pl
from jax.experimental.pallas import tpu as pltpu
from jax.sharding import PartitionSpec as P

D = 4096
HEAD = 64
QK = 32
SEQS = 4
PROP = 24
PAIRS = 4
LANES = 128
N_KV = 16
N_TP = 8
WINDOW = 48

f32 = jnp.float32
bf16 = jnp.bfloat16
epsilon = 1e-05
masked_low = -1e30
score_scale = QK ** (-0.5)
LOG2E = 1.4426950408889634

NT = (((1,), (1,)), ((), ()))
NN = (((1,), (0,)), ((), ()))


def iota(shape, dim):
    return lax.broadcasted_iota(jnp.int32, shape, dim)


def three_parts(row):
    wide = jnp.broadcast_to(row, (8, LANES))
    high = wide.astype(bf16).astype(f32)
    rest = wide - high
    middle = rest.astype(bf16).astype(f32)
    low = rest - middle
    place = iota((8, LANES), 0)
    tile = jnp.where(place == 0, high, jnp.where(place == 1, middle, jnp.where(place == 2, low, 0.0)))
    return tile.astype(bf16)


def column_to_row(column):
    count = column.shape[0]
    eye = iota((count, LANES), 0) == iota((count, LANES), 1)
    return jnp.sum(jnp.where(eye, column, 0.0), axis=0, keepdims=True)


def row_to_column(row, count):
    eye = iota((count, LANES), 0) == iota((count, LANES), 1)
    return jnp.sum(jnp.where(eye, row, 0.0), axis=1, keepdims=True)


def project_kernel(tokens, gain, w_query, w_key, w_value, out):
    wide = tokens[...].astype(f32)
    gained = (wide * gain[...]).astype(bf16)
    squares = jnp.sum(wide * wide, axis=1, keepdims=True)
    for place, weight in enumerate((w_query, w_key, w_value)):
        product = lax.dot_general(gained, weight[...], NN, preferred_element_type=f32).astype(bf16)
        for seq in range(SEQS):
            for pair in range(PAIRS):
                out[seq * PAIRS + pair, place * PROP : (place + 1) * PROP, :] = product[
                    seq * PROP : (seq + 1) * PROP, pair * LANES : (pair + 1) * LANES
                ]
    for seq in range(SEQS):
        tile = three_parts(column_to_row(squares[seq * PROP : (seq + 1) * PROP]))
        for pair in range(PAIRS):
            out[seq * PAIRS + pair, 3 * PROP :, :] = tile


def normalize_kernel(arrived, own, copies):
    total = arrived[0].astype(f32)
    for source in range(1, N_KV):
        total = total + arrived[source].astype(f32)
    row = total[72:73] + total[73:74] + total[74:75]
    factor = lax.rsqrt(row_to_column(row, PROP) / D + epsilon)
    for place in range(3):
        rows = slice(place * PROP, (place + 1) * PROP)
        part = (total[rows] * factor).astype(bf16)
        own[rows, :] = part
        for target in range(N_KV):
            copies[target, rows, :] = part


def expanded(queries, count):
    group = iota(queries.shape, 1) // QK
    zero = jnp.zeros_like(queries)
    return jnp.concatenate([jnp.where(group == place, queries, zero) for place in range(count)], axis=0)


def self_kernel(parents, own, out):
    pair_seq = lax.axis_index("kv") // PAIRS
    links = parents[pl.ds(pair_seq, 1), :].astype(f32)
    eye = (iota((PROP, PROP), 0) == iota((PROP, PROP), 1))
    column = jnp.sum(jnp.where(eye, jnp.broadcast_to(links, (PROP, PROP)), 0.0), axis=1, keepdims=True)
    reached = jnp.where(eye | (column == iota((PROP, PROP), 1).astype(f32)), 1.0, 0.0)
    for _ in range(5):
        narrow = reached.astype(bf16)
        reached = jnp.minimum(1.0, lax.dot_general(narrow, narrow, NN, preferred_element_type=f32))
    lineage = jnp.concatenate([reached] * 4, axis=0) > 0.5
    queries, keys, values = own[:PROP, :], own[PROP : 2 * PROP, :], own[2 * PROP :, :]
    scores = lax.dot_general(expanded(queries, 4), keys, NT, preferred_element_type=f32)
    scores = jnp.where(lineage, scores * score_scale, masked_low)
    largest = jnp.max(scores, axis=1, keepdims=True)
    weight = jnp.where(lineage, jnp.exp(scores - largest), 0.0)
    total = jnp.sum(weight, axis=1, keepdims=True)
    product = lax.dot_general(weight.astype(bf16), values, NN, preferred_element_type=f32) / total
    out[:48, :] = jnp.where(iota((48, LANES), 1) < HEAD, product[:48], product[48:])
    out[48:56, :] = jnp.broadcast_to(column_to_row(largest + jnp.log(total)), (8, LANES))


def attend_kernel(lengths, accepted, gathered, keys, values, out):
    seq, half = pl.program_id(0), pl.program_id(1)
    block_len = keys.shape[1]
    seen = lengths[seq] + accepted[seq] - lax.axis_index("kv") * block_len
    base = seq * PAIRS + half * 2
    queries = jnp.concatenate([gathered[base, :PROP, :], gathered[base + 1, :PROP, :]], axis=1)
    scores = lax.dot_general(expanded(queries, 8), keys[0], NT, preferred_element_type=f32)
    visible = iota((1, block_len), 1) < seen
    scores = jnp.where(visible, scores, masked_low)
    largest = jnp.max(scores, axis=1, keepdims=True)
    weight = jnp.exp2((scores - largest) * (score_scale * LOG2E))
    total = jnp.sum(weight, axis=1, keepdims=True)
    product = lax.dot_general(weight.astype(bf16), values[0], NN, preferred_element_type=f32) / total
    lane_head = iota((48, 2 * LANES), 1) // HEAD
    merged = jnp.where(lane_head == 0, product[:48], 0.0)
    for head in range(1, 4):
        merged = jnp.where(lane_head == head, product[head * 48 : (head + 1) * 48], merged)
    merged = merged.astype(bf16)
    level = jnp.where(seen > 0, largest * score_scale + jnp.log(total), masked_low)
    for pair in range(2):
        out[pair, :48, :] = merged[:, pair * LANES : (pair + 1) * LANES]
        out[pair, 48:, :] = three_parts(column_to_row(level[pair * 96 : (pair + 1) * 96]))


def finish_kernel(map_lambda, out_gain, arrived, own_part, copies):
    pair = lax.axis_index("kv") % PAIRS
    rows = []
    for source in range(N_KV):
        tile = arrived[source, 48:, :].astype(f32)
        rows.append(tile[0:1] + tile[1:2] + tile[2:3])
    rows.append(own_part[48:49, :])
    levels = jnp.concatenate(rows + [jnp.full((7, LANES), masked_low, f32)], axis=0)
    weights = jnp.exp(levels - jnp.max(levels, axis=0, keepdims=True))
    weights = weights / jnp.sum(weights, axis=0, keepdims=True)
    columns = jnp.concatenate([weights, jnp.zeros((LANES - 24, LANES), f32)], axis=0).T
    first = iota((48, LANES), 1) < HEAD
    total = jnp.zeros((48, LANES), f32)
    for source in range(N_KV + 1):
        factor = jnp.where(first, columns[:48, source : source + 1], columns[48:96, source : source + 1])
        part = arrived[source, :48, :].astype(f32) if source < N_KV else own_part[:48, :]
        total = total + factor * part
    lane_first = iota((PROP, LANES), 1) < HEAD
    lam = jnp.where(lane_first, map_lambda[2 * pair], map_lambda[2 * pair + 1])
    difference = total[:PROP] - lam * total[PROP:]
    squared = difference * difference
    mean_first = jnp.sum(jnp.where(lane_first, squared, 0.0), axis=1, keepdims=True)
    mean_second = jnp.sum(jnp.where(lane_first, 0.0, squared), axis=1, keepdims=True)
    mean = jnp.where(lane_first, mean_first, mean_second) / HEAD
    normed = (difference * lax.rsqrt(mean + epsilon) * out_gain[pl.ds(pair, 1), :]).astype(bf16)
    for target in range(N_KV):
        copies[target] = normed


def output_kernel(arrived, w_output, copies):
    total = None
    for pair in range(PAIRS):
        rows = jnp.concatenate([arrived[seq * PAIRS + pair] for seq in range(SEQS)], axis=0)
        part = lax.dot_general(
            rows, w_output[pair * LANES : (pair + 1) * LANES, :], NN, preferred_element_type=f32
        )
        total = part if total is None else total + part
    total = total.astype(bf16)
    for target in range(N_TP):
        copies[target] = total


def mix_kernel(arrived, out):
    total = arrived[0].astype(f32)
    for source in range(1, N_TP):
        total = total + arrived[source].astype(f32)
    out[...] = total.astype(bf16)


def write_kernel(lengths, accepted, gathered, keys, values, new_keys, new_values):
    seq = pl.program_id(0)
    block_len = keys.shape[1]
    begin = lengths[seq] + accepted[seq] - lax.axis_index("kv") * block_len
    new_keys[...] = keys[...]
    new_values[...] = values[...]

    @pl.when((begin > -PROP) & (begin < block_len))
    def _():
        base = pl.multiple_of(jnp.clip((begin // 16) * 16, 0, block_len - WINDOW), 16)
        slot = base - begin + iota((WINDOW, PROP), 0)
        placing = (slot == iota((WINDOW, PROP), 1)).astype(bf16)
        row = base - begin + iota((WINDOW, LANES), 0)
        written = (row >= 0) & (row < PROP)
        for place, target in ((1, new_keys), (2, new_values)):
            for pair in range(PAIRS):
                lanes = slice(pair * LANES, (pair + 1) * LANES)
                rows = gathered[seq * PAIRS + pair, place * PROP : (place + 1) * PROP, :]
                moved = lax.dot_general(placing, rows, NN, preferred_element_type=f32)
                old = target[0, pl.ds(base, WINDOW), lanes]
                target[0, pl.ds(base, WINDOW), lanes] = jnp.where(written, moved, old.astype(f32)).astype(bf16)


def vmem():
    return pl.BlockSpec(memory_space=pltpu.VMEM)


def smem():
    return pl.BlockSpec(memory_space=pltpu.SMEM)


def shape(dims, kind=bf16):
    return jax.ShapeDtypeStruct(dims, kind)


def room(mebibytes):
    return pltpu.CompilerParams(vmem_limit_bytes=mebibytes * 1024 * 1024)


def cost(flops, moved):
    return pl.CostEstimate(flops=flops, bytes_accessed=moved, transcendentals=0)


def local(
    tokens,
    norm_gain,
    w_query,
    w_key,
    w_value,
    w_output,
    cache_keys,
    cache_values,
    map_lambda,
    out_gain,
    parents,
    lengths,
    accepted,
):
    block_len = cache_keys.shape[1]
    width = cache_keys.shape[2]
    exchange = functools.partial(lax.all_to_all, split_axis=0, concat_axis=0, tiled=True)

    partial = pl.pallas_call(
        project_kernel,
        out_shape=shape((N_KV, 80, LANES)),
        in_specs=[vmem()] * 5,
        out_specs=vmem(),
        compiler_params=room(8),
        name="project",
    )(tokens, norm_gain.reshape(1, -1), w_query, w_key, w_value)
    arrived = exchange(partial, "kv")
    own, copies = pl.pallas_call(
        normalize_kernel,
        out_shape=(shape((72, LANES)), shape((N_KV, 72, LANES))),
        in_specs=[vmem()],
        out_specs=(vmem(), vmem()),
        compiler_params=room(8),
        name="normalize",
    )(arrived)
    gathered = exchange(copies, "kv")
    own_part = pl.pallas_call(
        self_kernel,
        out_shape=shape((56, LANES), f32),
        in_specs=[vmem(), vmem()],
        out_specs=vmem(),
        cost_estimate=cost(4_000_000_000, 100_000),
        compiler_params=room(8),
        name="own_scores",
    )(parents, own)
    cache_block = pl.BlockSpec((1, block_len, 2 * LANES), lambda seq, half: (seq, 0, half))
    parts = pl.pallas_call(
        attend_kernel,
        grid=(SEQS, 2),
        out_shape=shape((N_KV, 56, LANES)),
        in_specs=[smem(), smem(), vmem(), cache_block, cache_block],
        out_specs=pl.BlockSpec((2, 56, LANES), lambda seq, half: (seq * 2 + half, 0, 0)),
        compiler_params=room(16),
        name="attend",
    )(lengths, accepted, gathered, cache_keys, cache_values)
    arrived_parts = exchange(parts, "kv")
    whole = pl.BlockSpec((1, block_len, width), lambda seq: (seq, 0, 0))
    new_keys, new_values = pl.pallas_call(
        write_kernel,
        grid=(SEQS,),
        out_shape=(shape(cache_keys.shape), shape(cache_values.shape)),
        in_specs=[smem(), smem(), vmem(), whole, whole],
        out_specs=(whole, whole),
        cost_estimate=cost(8_000_000_000, 8_000_000),
        compiler_params=room(16),
        name="write",
    )(lengths, accepted, gathered, cache_keys, cache_values)
    normed = pl.pallas_call(
        finish_kernel,
        out_shape=shape((N_KV, PROP, LANES)),
        in_specs=[smem(), vmem(), vmem(), vmem()],
        out_specs=vmem(),
        compiler_params=room(8),
        name="finish",
    )(map_lambda, out_gain.reshape(PAIRS, LANES), arrived_parts, own_part)
    arrived_normed = exchange(normed, "kv")
    partial_out = pl.pallas_call(
        output_kernel,
        out_shape=shape((N_TP, SEQS * PROP, w_output.shape[1])),
        in_specs=[vmem(), vmem()],
        out_specs=vmem(),
        compiler_params=room(8),
        name="output",
    )(arrived_normed, w_output)
    arrived_out = exchange(partial_out, "tp")
    mixed = pl.pallas_call(
        mix_kernel,
        out_shape=shape((SEQS * PROP, w_output.shape[1])),
        in_specs=[vmem()],
        out_specs=vmem(),
        compiler_params=room(8),
        name="mix",
    )(arrived_out)
    return (mixed, new_keys, new_values)


def solution(mesh):
    return jax.shard_map(
        local,
        mesh=mesh,
        in_specs=(
            P(None, "kv"),
            P("kv"),
            P("kv", "tp"),
            P("kv", "tp"),
            P("kv", "tp"),
            P("tp", "kv"),
            P(None, "kv", "tp"),
            P(None, "kv", "tp"),
            P("tp"),
            P("tp"),
            P(),
            P(),
            P(),
        ),
        out_specs=(P(None, "kv"), P(None, "kv", "tp"), P(None, "kv", "tp")),
        check_vma=False,
    )
```

```python
import functools

import jax
import jax.numpy as jnp
from jax import lax
from jax.experimental import pallas as pl
from jax.experimental.pallas import tpu as pltpu
from jax.sharding import PartitionSpec as P

D = 4096
HEAD = 64
QK = 32
SEQS = 4
PROP = 24
PAIRS = 4
LANES = 128
N_KV = 16
N_TP = 8
WINDOW = 48

f32 = jnp.float32
bf16 = jnp.bfloat16
epsilon = 1e-05
masked_low = -1e30
score_scale = QK ** (-0.5)
LOG2E = 1.4426950408889634

NT = (((1,), (1,)), ((), ()))
NN = (((1,), (0,)), ((), ()))


def iota(shape, dim):
    return lax.broadcasted_iota(jnp.int32, shape, dim)


def three_parts(row):
    wide = jnp.broadcast_to(row, (8, LANES))
    high = wide.astype(bf16).astype(f32)
    rest = wide - high
    middle = rest.astype(bf16).astype(f32)
    low = rest - middle
    place = iota((8, LANES), 0)
    tile = jnp.where(place == 0, high, jnp.where(place == 1, middle, jnp.where(place == 2, low, 0.0)))
    return tile.astype(bf16)


def column_to_row(column):
    count = column.shape[0]
    eye = iota((count, LANES), 0) == iota((count, LANES), 1)
    return jnp.sum(jnp.where(eye, column, 0.0), axis=0, keepdims=True)


def row_to_column(row, count):
    eye = iota((count, LANES), 0) == iota((count, LANES), 1)
    return jnp.sum(jnp.where(eye, row, 0.0), axis=1, keepdims=True)


def project_kernel(tokens_far, gain_far, query_far, key_far, value_far, out, tokens, gain, query, key, value, done):
    far = (tokens_far, gain_far, query_far, key_far, value_far)
    near = (tokens, gain, query, key, value)
    loads = [pltpu.make_async_copy(a, b, done.at[place]) for place, (a, b) in enumerate(zip(far, near))]
    for load in loads:
        load.start()
    loads[0].wait()
    loads[1].wait()
    wide = tokens[...].astype(f32)
    gained = (wide * gain[...]).astype(bf16)
    squares = jnp.sum(wide * wide, axis=1, keepdims=True)
    for place, weight in enumerate((query, key, value)):
        loads[2 + place].wait()
        product = lax.dot_general(gained, weight[...], NN, preferred_element_type=f32).astype(bf16)
        for seq in range(SEQS):
            for pair in range(PAIRS):
                out[seq * PAIRS + pair, place * PROP : (place + 1) * PROP, :] = product[
                    seq * PROP : (seq + 1) * PROP, pair * LANES : (pair + 1) * LANES
                ]
    for seq in range(SEQS):
        tile = three_parts(column_to_row(squares[seq * PROP : (seq + 1) * PROP]))
        for pair in range(PAIRS):
            out[seq * PAIRS + pair, 3 * PROP :, :] = tile


def normalize_kernel(arrived, own, copies):
    total = arrived[0].astype(f32)
    for source in range(1, N_KV):
        total = total + arrived[source].astype(f32)
    row = total[72:73] + total[73:74] + total[74:75]
    factor = lax.rsqrt(row_to_column(row, PROP) / D + epsilon)
    for place in range(3):
        rows = slice(place * PROP, (place + 1) * PROP)
        part = (total[rows] * factor).astype(bf16)
        own[rows, :] = part
        for target in range(N_KV):
            copies[target, rows, :] = part


def expanded(queries, count):
    group = iota(queries.shape, 1) // QK
    zero = jnp.zeros_like(queries)
    return jnp.concatenate([jnp.where(group == place, queries, zero) for place in range(count)], axis=0)


def own_scores(parents, own, out):
    pair_seq = lax.axis_index("kv") // PAIRS
    links = parents[pl.ds(pair_seq, 1), :].astype(f32)
    eye = (iota((PROP, PROP), 0) == iota((PROP, PROP), 1))
    column = jnp.sum(jnp.where(eye, jnp.broadcast_to(links, (PROP, PROP)), 0.0), axis=1, keepdims=True)
    reached = jnp.where(eye | (column == iota((PROP, PROP), 1).astype(f32)), 1.0, 0.0)
    for _ in range(5):
        narrow = reached.astype(bf16)
        reached = jnp.minimum(1.0, lax.dot_general(narrow, narrow, NN, preferred_element_type=f32))
    lineage = jnp.concatenate([reached] * 4, axis=0) > 0.5
    queries, keys, values = own[:PROP, :], own[PROP : 2 * PROP, :], own[2 * PROP :, :]
    scores = lax.dot_general(expanded(queries, 4), keys, NT, preferred_element_type=f32)
    scores = jnp.where(lineage, scores * score_scale, masked_low)
    largest = jnp.max(scores, axis=1, keepdims=True)
    weight = jnp.where(lineage, jnp.exp(scores - largest), 0.0)
    total = jnp.sum(weight, axis=1, keepdims=True)
    product = lax.dot_general(weight.astype(bf16), values, NN, preferred_element_type=f32) / total
    out[:48, :] = jnp.where(iota((48, LANES), 1) < HEAD, product[:48], product[48:])
    out[48:56, :] = jnp.broadcast_to(column_to_row(largest + jnp.log(total)), (8, LANES))


def attend_kernel(
    lengths,
    accepted,
    gathered,
    keys,
    values_far,
    parents,
    own,
    out,
    new_keys,
    new_values,
    own_part,
    values,
    window,
    loaded,
    stored,
    patched,
):
    block_len = keys.shape[1]
    offset = lax.axis_index("kv") * block_len
    loads = [pltpu.make_async_copy(values_far.at[seq], values.at[seq], loaded.at[seq]) for seq in range(SEQS)]
    stores = [
        pltpu.make_async_copy(source.at[seq], target.at[seq], stored.at[seq, place])
        for seq in range(SEQS)
        for place, (source, target) in enumerate(((keys, new_keys), (values, new_values)))
    ]
    for load in loads:
        load.start()
    begins = [lengths[seq] + accepted[seq] - offset for seq in range(SEQS)]
    bases = [pl.multiple_of(jnp.clip((begin // 16) * 16, 0, block_len - WINDOW), 16) for begin in begins]
    here = [(begin > -PROP) & (begin < block_len) for begin in begins]

    def patches(seq):
        return [
            pltpu.make_async_copy(
                window.at[seq, place], target.at[seq, pl.ds(bases[seq], WINDOW)], patched.at[seq, place]
            )
            for place, target in enumerate((new_keys, new_values))
        ]

    lane_head = iota((48, 2 * LANES), 1) // HEAD
    for seq in range(SEQS):
        stores[2 * seq].start()
        visible = iota((1, block_len), 1) < begins[seq]
        weights = []
        for half in range(2):
            base = seq * PAIRS + half * 2
            lanes = slice(half * 2 * LANES, (half + 1) * 2 * LANES)
            queries = jnp.concatenate([gathered[base, :PROP, :], gathered[base + 1, :PROP, :]], axis=1)
            scores = lax.dot_general(expanded(queries, 8), keys[seq, :, lanes], NT, preferred_element_type=f32)
            scores = jnp.where(visible, scores, masked_low)
            largest = jnp.max(scores, axis=1, keepdims=True)
            weight = jnp.exp2((scores - largest) * (score_scale * LOG2E))
            total = jnp.sum(weight, axis=1, keepdims=True)
            level = jnp.where(begins[seq] > 0, largest * score_scale + jnp.log(total), masked_low)
            for pair in range(2):
                out[base + pair, 48:, :] = three_parts(column_to_row(level[pair * 96 : (pair + 1) * 96]))
            weights.append((weight.astype(bf16), 1.0 / total))
        loads[seq].wait()
        stores[2 * seq + 1].start()
        for half in range(2):
            base = seq * PAIRS + half * 2
            lanes = slice(half * 2 * LANES, (half + 1) * 2 * LANES)
            weight, inverse = weights[half]
            product = lax.dot_general(weight, values[seq, :, lanes], NN, preferred_element_type=f32)
            merged = jnp.where(lane_head == 0, product[:48] * inverse[:48], 0.0)
            for head in range(1, 4):
                rows = slice(head * 48, (head + 1) * 48)
                merged = jnp.where(lane_head == head, product[rows] * inverse[rows], merged)
            merged = merged.astype(bf16)
            for pair in range(2):
                out[base + pair, :48, :] = merged[:, pair * LANES : (pair + 1) * LANES]
    for seq in range(SEQS):

        @pl.when(here[seq])
        def _():
            shift = bases[seq] - begins[seq]
            placing = (shift + iota((WINDOW, PROP), 0) == iota((WINDOW, PROP), 1)).astype(bf16)
            row = shift + iota((WINDOW, LANES), 0)
            written = (row >= 0) & (row < PROP)
            for place, source in ((0, keys), (1, values)):
                for pair in range(PAIRS):
                    lanes = slice(pair * LANES, (pair + 1) * LANES)
                    rows = gathered[seq * PAIRS + pair, (place + 1) * PROP : (place + 2) * PROP, :]
                    moved = lax.dot_general(placing, rows, NN, preferred_element_type=f32)
                    old = source[seq, pl.ds(bases[seq], WINDOW), lanes].astype(f32)
                    window[seq, place, :, lanes] = jnp.where(written, moved, old).astype(bf16)

    for store in stores:
        store.wait()
    for seq in range(SEQS):

        @pl.when(here[seq])
        def _():
            for patch in patches(seq):
                patch.start()

    own_scores(parents, own, own_part)
    for seq in range(SEQS):

        @pl.when(here[seq])
        def _():
            for patch in patches(seq):
                patch.wait()


def finish_kernel(map_lambda, out_gain, arrived, own_part, copies):
    pair = lax.axis_index("kv") % PAIRS
    rows = []
    for source in range(N_KV):
        tile = arrived[source, 48:, :].astype(f32)
        rows.append(tile[0:1] + tile[1:2] + tile[2:3])
    rows.append(own_part[48:49, :])
    levels = jnp.concatenate(rows + [jnp.full((7, LANES), masked_low, f32)], axis=0)
    weights = jnp.exp(levels - jnp.max(levels, axis=0, keepdims=True))
    weights = weights / jnp.sum(weights, axis=0, keepdims=True)
    columns = jnp.concatenate([weights, jnp.zeros((LANES - 24, LANES), f32)], axis=0).T
    first = iota((48, LANES), 1) < HEAD
    total = jnp.zeros((48, LANES), f32)
    for source in range(N_KV + 1):
        factor = jnp.where(first, columns[:48, source : source + 1], columns[48:96, source : source + 1])
        part = arrived[source, :48, :].astype(f32) if source < N_KV else own_part[:48, :]
        total = total + factor * part
    lane_first = iota((PROP, LANES), 1) < HEAD
    lam = jnp.where(lane_first, map_lambda[2 * pair], map_lambda[2 * pair + 1])
    difference = total[:PROP] - lam * total[PROP:]
    squared = difference * difference
    mean_first = jnp.sum(jnp.where(lane_first, squared, 0.0), axis=1, keepdims=True)
    mean_second = jnp.sum(jnp.where(lane_first, 0.0, squared), axis=1, keepdims=True)
    mean = jnp.where(lane_first, mean_first, mean_second) / HEAD
    normed = (difference * lax.rsqrt(mean + epsilon) * out_gain[pl.ds(pair, 1), :]).astype(bf16)
    for target in range(N_KV):
        copies[target] = normed


def output_kernel(arrived, w_output, copies):
    total = None
    for pair in range(PAIRS):
        rows = jnp.concatenate([arrived[seq * PAIRS + pair] for seq in range(SEQS)], axis=0)
        part = lax.dot_general(
            rows, w_output[pair * LANES : (pair + 1) * LANES, :], NN, preferred_element_type=f32
        )
        total = part if total is None else total + part
    total = total.astype(bf16)
    for target in range(N_TP):
        copies[target] = total


def mix_kernel(arrived, out):
    total = arrived[0].astype(f32)
    for source in range(1, N_TP):
        total = total + arrived[source].astype(f32)
    out[...] = total.astype(bf16)


def vmem():
    return pl.BlockSpec(memory_space=pltpu.VMEM)


def hbm():
    return pl.BlockSpec(memory_space=pltpu.HBM)


def smem():
    return pl.BlockSpec(memory_space=pltpu.SMEM)


def shape(dims, kind=bf16):
    return jax.ShapeDtypeStruct(dims, kind)


def room(mebibytes):
    return pltpu.CompilerParams(vmem_limit_bytes=mebibytes * 1024 * 1024)


def near(dims, kind=bf16):
    return pltpu.VMEM(dims, kind)


def far(*arrays):
    return [pltpu.with_memory_space_constraint(array, pltpu.HBM) for array in arrays]


def cost(flops, moved):
    return pl.CostEstimate(flops=flops, bytes_accessed=moved, transcendentals=0)


def local(
    tokens,
    norm_gain,
    w_query,
    w_key,
    w_value,
    w_output,
    cache_keys,
    cache_values,
    map_lambda,
    out_gain,
    parents,
    lengths,
    accepted,
):
    width = cache_keys.shape[2]
    exchange = functools.partial(lax.all_to_all, split_axis=0, concat_axis=0, tiled=True)

    partial = pl.pallas_call(
        project_kernel,
        out_shape=near((N_KV, 80, LANES)),
        in_specs=[hbm()] * 5,
        out_specs=vmem(),
        scratch_shapes=[
            pltpu.VMEM(tokens.shape, bf16),
            pltpu.VMEM((1, norm_gain.shape[0]), f32),
            pltpu.VMEM(w_query.shape, bf16),
            pltpu.VMEM(w_key.shape, bf16),
            pltpu.VMEM(w_value.shape, bf16),
            pltpu.SemaphoreType.DMA((5,)),
        ],
        compiler_params=room(8),
        name="project",
    )(*far(tokens, norm_gain.reshape(1, -1), w_query, w_key, w_value))
    near_keys = pltpu.with_memory_space_constraint(cache_keys, pltpu.VMEM)
    arrived = exchange(partial, "kv")
    own, copies = pl.pallas_call(
        normalize_kernel,
        out_shape=(near((72, LANES)), near((N_KV, 72, LANES))),
        in_specs=[vmem()],
        out_specs=(vmem(), vmem()),
        compiler_params=room(8),
        name="normalize",
    )(arrived)
    gathered = exchange(copies, "kv")
    parts, new_keys, new_values, own_part = pl.pallas_call(
        attend_kernel,
        out_shape=(
            near((N_KV, 56, LANES)),
            shape(cache_keys.shape),
            shape(cache_values.shape),
            near((56, LANES), f32),
        ),
        in_specs=[smem(), smem(), vmem(), vmem(), hbm(), vmem(), vmem()],
        out_specs=(vmem(), hbm(), hbm(), vmem()),
        scratch_shapes=[
            pltpu.VMEM(cache_values.shape, bf16),
            pltpu.VMEM((SEQS, 2, WINDOW, width), bf16),
            pltpu.SemaphoreType.DMA((SEQS,)),
            pltpu.SemaphoreType.DMA((SEQS, 2)),
            pltpu.SemaphoreType.DMA((SEQS, 2)),
        ],
        compiler_params=room(24),
        name="attend",
    )(lengths, accepted, gathered, near_keys, *far(cache_values), parents, own)
    arrived_parts = exchange(parts, "kv")
    normed = pl.pallas_call(
        finish_kernel,
        out_shape=near((N_KV, PROP, LANES)),
        in_specs=[smem(), vmem(), vmem(), vmem()],
        out_specs=vmem(),
        compiler_params=room(8),
        name="finish",
    )(map_lambda, out_gain.reshape(PAIRS, LANES), arrived_parts, own_part)
    arrived_normed = exchange(normed, "kv")
    partial_out = pl.pallas_call(
        output_kernel,
        out_shape=near((N_TP, SEQS * PROP, w_output.shape[1])),
        in_specs=[vmem(), vmem()],
        out_specs=vmem(),
        compiler_params=room(8),
        name="output",
    )(arrived_normed, w_output)
    arrived_out = exchange(partial_out, "tp")
    mixed = pl.pallas_call(
        mix_kernel,
        out_shape=shape((SEQS * PROP, w_output.shape[1])),
        in_specs=[vmem()],
        out_specs=vmem(),
        compiler_params=room(8),
        name="mix",
    )(arrived_out)
    return (mixed, new_keys, new_values)


def solution(mesh):
    return jax.shard_map(
        local,
        mesh=mesh,
        in_specs=(
            P(None, "kv"),
            P("kv"),
            P("kv", "tp"),
            P("kv", "tp"),
            P("kv", "tp"),
            P("tp", "kv"),
            P(None, "kv", "tp"),
            P(None, "kv", "tp"),
            P("tp"),
            P("tp"),
            P(),
            P(),
            P(),
        ),
        out_specs=(P(None, "kv"), P(None, "kv", "tp"), P(None, "kv", "tp")),
        check_vma=False,
    )
```

```python
import functools

import jax
import jax.numpy as jnp
from jax import lax
from jax.experimental import pallas as pl
from jax.experimental.pallas import tpu as pltpu
from jax.sharding import PartitionSpec as P

D = 4096
HEAD = 64
QK = 32
SEQS = 4
PROP = 24
PAIRS = 4
LANES = 128
N_KV = 16
N_TP = 8
WINDOW = 48
LAG = 3

f32 = jnp.float32
bf16 = jnp.bfloat16
epsilon = 1e-05
masked_low = -1e30
score_scale = QK ** (-0.5)
LOG2E = 1.4426950408889634

NT = (((1,), (1,)), ((), ()))
NN = (((1,), (0,)), ((), ()))


def iota(shape, dim):
    return lax.broadcasted_iota(jnp.int32, shape, dim)


def three_parts(first, second):
    place = iota((8, LANES), 0)
    wide = jnp.where(place % 2 == 0, first, second)
    high = wide.astype(bf16).astype(f32)
    rest = wide - high
    middle = rest.astype(bf16).astype(f32)
    low = rest - middle
    tile = jnp.where(place < 2, high, jnp.where(place < 4, middle, jnp.where(place < 6, low, 0.0)))
    return tile.astype(bf16)


def column_to_row(column):
    count = column.shape[0]
    eye = iota((count, LANES), 0) == iota((count, LANES), 1)
    return jnp.sum(jnp.where(eye, column, 0.0), axis=0, keepdims=True)


def row_to_column(row, count):
    eye = iota((count, LANES), 0) == iota((count, LANES), 1)
    return jnp.sum(jnp.where(eye, row, 0.0), axis=1, keepdims=True)


def project_kernel(
    tokens_far,
    gain_far,
    query_far,
    key_far,
    value_far,
    out,
    tokens,
    gain,
    query,
    key,
    value,
    done,
):
    far = (tokens_far, gain_far, query_far, key_far, value_far)
    near = (tokens, gain, query, key, value)
    loads = [pltpu.make_async_copy(a, b, done.at[place]) for place, (a, b) in enumerate(zip(far, near))]
    for load in loads:
        load.start()
    for load in loads[:2]:
        load.wait()
    wide = tokens[...].astype(f32)
    gained = (wide * gain[...]).astype(bf16)
    squares = jnp.sum(wide * wide, axis=1, keepdims=True)
    for seq in range(SEQS):
        row = column_to_row(squares[seq * PROP : (seq + 1) * PROP])
        tile = three_parts(row, row)
        for pair in range(PAIRS):
            out[seq * PAIRS + pair, 3 * PROP :, :] = tile
    for place, weight in enumerate((query, key, value)):
        loads[2 + place].wait()
        product = lax.dot_general(gained, weight[...], NN, preferred_element_type=f32).astype(bf16)
        for seq in range(SEQS):
            for pair in range(PAIRS):
                out[seq * PAIRS + pair, place * PROP : (place + 1) * PROP, :] = product[
                    seq * PROP : (seq + 1) * PROP, pair * LANES : (pair + 1) * LANES
                ]


def normalize_kernel(arrived, own, copies):
    total = arrived[0].astype(f32)
    for source in range(1, N_KV):
        total = total + arrived[source].astype(f32)
    row = total[72:73] + total[74:75] + total[76:77]
    factor = lax.rsqrt(row_to_column(row, PROP) / D + epsilon)
    for place in range(3):
        rows = slice(place * PROP, (place + 1) * PROP)
        scaled = factor * (score_scale * LOG2E) if place == 0 else factor
        part = (total[rows] * scaled).astype(bf16)
        own[rows, :] = part
        for target in range(N_KV):
            copies[target, rows, :] = part


def expanded(queries):
    group = iota(queries.shape, 1) // QK
    zero = jnp.zeros_like(queries)
    return jnp.concatenate([jnp.where(group == place, queries, zero) for place in range(4)], axis=0)


def by_head(array):
    return jnp.where(iota((48, LANES), 1) < HEAD, array[:48], array[48:])


def own_steps(parents, own, out):
    eye = iota((PROP, PROP), 0) == iota((PROP, PROP), 1)
    links = parents[pl.ds(lax.axis_index("kv") // PAIRS, 1), :].astype(f32)
    column = jnp.sum(jnp.where(eye, links, 0.0), axis=1, keepdims=True)
    reached = jnp.where(eye | (column == iota((PROP, PROP), 1).astype(f32)), 1.0, 0.0)
    queries, keys, values = own[:PROP, :], own[PROP : 2 * PROP, :], own[2 * PROP :, :]
    scores = lax.dot_general(expanded(queries), keys, NT, preferred_element_type=f32)
    yield
    for _ in range(5):
        narrow = reached.astype(bf16)
        reached = jnp.minimum(1.0, lax.dot_general(narrow, narrow, NN, preferred_element_type=f32))
        yield
    related = jnp.concatenate([reached] * 4, axis=0) > 0.5
    scores = jnp.where(related, scores, masked_low)
    largest = jnp.max(scores, axis=1, keepdims=True)
    yield
    weight = jnp.where(related, jnp.exp2(scores - largest), 0.0)
    total = jnp.sum(weight, axis=1, keepdims=True)
    yield
    product = lax.dot_general(weight.astype(bf16), values, NN, preferred_element_type=f32)
    yield
    out[:48, :] = by_head(product / total)
    out[48:, :] = by_head(jnp.broadcast_to(largest + jnp.log2(total), (96, LANES)))
    yield


def attend_kernel(
    lengths,
    accepted,
    gathered,
    keys,
    values,
    out_far,
    out,
    sent,
):
    block_len = keys.shape[1]
    ends = lengths[...] + accepted[...] - lax.axis_index("kv") * block_len
    sends = [
        pltpu.make_async_copy(
            out.at[pl.ds(seq * PAIRS, PAIRS)], out_far.at[pl.ds(seq * PAIRS, PAIRS)], sent.at[seq]
        )
        for seq in range(SEQS)
    ]
    def scored(seq, pair):
        lanes = slice(pair * LANES, (pair + 1) * LANES)
        queries = expanded(gathered[seq * PAIRS + pair, :PROP, :])
        return lax.dot_general(queries, keys[seq, :, lanes], NT, preferred_element_type=f32)

    def weighed(seq, scores):
        visible = iota((1, block_len), 1) < ends[:, seq : seq + 1]
        scores = jnp.where(visible, scores, masked_low)
        largest = jnp.max(scores, axis=1, keepdims=True)
        return largest, jnp.exp2(scores - largest).astype(bf16)

    ones = jnp.ones((block_len, LANES), bf16)
    eye = iota((48, LANES), 0) == iota((48, LANES), 1)

    def finished(seq, pair, largest, weight):
        lanes = slice(pair * LANES, (pair + 1) * LANES)
        both = jnp.concatenate([values[seq, :, lanes], ones], axis=1)
        product = lax.dot_general(weight, both, NN, preferred_element_type=f32)
        total = product[:, LANES:]
        out[seq * PAIRS + pair, :48, :] = by_head(product[:, :LANES] / total).astype(bf16)
        level = largest + jnp.log2(total)
        first = jnp.sum(jnp.where(eye, level[:48], 0.0), axis=0, keepdims=True)
        second = jnp.sum(jnp.where(eye, level[48:], 0.0), axis=0, keepdims=True)
        seen = ends[:, seq : seq + 1] > 0
        tile = three_parts(jnp.where(seen, first, masked_low), jnp.where(seen, second, masked_low))
        out[seq * PAIRS + pair, 48:, :] = tile

    units = [(seq, pair) for seq in range(SEQS) for pair in range(PAIRS)]
    scores = scored(*units[0])
    waiting = []
    for place in range(len(units) + LAG):
        if place < len(units):
            following = scored(*units[place + 1]) if place + 1 < len(units) else None
            waiting.append((units[place], weighed(units[place][0], scores)))
            scores = following
        if place >= LAG:
            (seq, pair), found = waiting.pop(0)
            finished(seq, pair, *found)
            if pair == PAIRS - 1:
                sends[seq].start()
    for send in sends:
        send.wait()


def write_kernel(
    lengths,
    accepted,
    gathered,
    parents,
    own,
    keys_far,
    values_far,
    new_keys,
    new_values,
    own_part,
    keys,
    values,
    window,
    loaded,
    stored,
    patched,
):
    block_len = keys.shape[1]
    offset = lax.axis_index("kv") * block_len
    pieces = [
        (seq, place, source, middle, target)
        for seq in range(SEQS)
        for place, (source, middle, target) in enumerate(
            ((keys_far, keys, new_keys), (values_far, values, new_values))
        )
    ]
    loads = [pltpu.make_async_copy(a.at[seq], b.at[seq], loaded.at[seq, place]) for seq, place, a, b, _ in pieces]
    stores = [pltpu.make_async_copy(b.at[seq], c.at[seq], stored.at[seq, place]) for seq, place, _, b, c in pieces]
    for load in loads:
        load.start()
    for _ in own_steps(parents, own, own_part):
        pass
    for load, store in zip(loads, stores):
        load.wait()
        store.start()

    def patch(seq):
        begin = lengths[seq] + accepted[seq] - offset
        base = pl.multiple_of(jnp.clip((begin // 16) * 16, 0, block_len - WINDOW), 16)
        copies = [
            pltpu.make_async_copy(
                window.at[seq, place], target.at[seq, pl.ds(base, WINDOW)], patched.at[seq, place]
            )
            for place, target in enumerate((new_keys, new_values))
        ]
        here = (begin > -PROP) & (begin < block_len)

        @pl.when(here)
        def _():
            shift = base - begin
            placing = (shift + iota((WINDOW, PROP), 0) == iota((WINDOW, PROP), 1)).astype(bf16)
            row = shift + iota((WINDOW, PAIRS * LANES), 0)
            written = (row >= 0) & (row < PROP)
            for place, source in ((0, keys), (1, values)):
                rows = jnp.concatenate(
                    [
                        gathered[seq * PAIRS + pair, (place + 1) * PROP : (place + 2) * PROP, :]
                        for pair in range(PAIRS)
                    ],
                    axis=1,
                )
                moved = lax.dot_general(placing, rows, NN, preferred_element_type=f32)
                old = source[seq, pl.ds(base, WINDOW), :].astype(f32)
                window[seq, place] = jnp.where(written, moved, old).astype(bf16)
            for place in range(2):
                stores[2 * seq + place].wait()
                copies[place].start()

        @pl.when(jnp.logical_not(here))
        def _():
            for place in range(2):
                stores[2 * seq + place].wait()

        return here, copies

    for here, copies in [patch(seq) for seq in range(SEQS)]:

        @pl.when(here)
        def _():
            for copy in copies:
                copy.wait()


def finish_kernel(map_lambda, out_gain, arrived, own_part, copies):
    pair = lax.axis_index("kv") % PAIRS
    lane = iota((48, LANES), 1)
    levels = jnp.concatenate([arrived[source, 48:, :].astype(f32) for source in range(N_KV)], axis=0).T[:48]
    levels = levels + pltpu.roll(levels, LANES - 2, 1) + pltpu.roll(levels, LANES - 4, 1)
    own_level = own_part[48:, :]
    is_first, is_second = lane % 8 == 0, lane % 8 == 1
    top = [
        jnp.maximum(
            jnp.max(jnp.where(mine, levels, masked_low), axis=1, keepdims=True), own_level[:, spot : spot + 1]
        )
        for mine, spot in ((is_first, 0), (is_second, HEAD))
    ]
    weights = jnp.exp2(jnp.where(is_first, levels - top[0], jnp.where(is_second, levels - top[1], masked_low)))
    own_weight = jnp.exp2(own_level - jnp.where(lane < HEAD, top[0], top[1]))
    sums = [jnp.sum(jnp.where(mine, weights, 0.0), axis=1, keepdims=True) for mine in (is_first, is_second)]
    whole = jnp.where(lane < HEAD, sums[0], sums[1]) + own_weight
    total = own_weight * own_part[:48, :]
    spot = jnp.where(lane < HEAD, 0, 1)
    for source in range(N_KV):
        factor = jnp.take_along_axis(weights, spot + 8 * source, axis=1, mode="promise_in_bounds")
        total = total + factor * arrived[source, :48, :].astype(f32)
    total = total / whole
    lane_first = iota((PROP, LANES), 1) < HEAD
    heads = iota((1, 8), 1) - 2 * pair
    lams = [jnp.sum(jnp.where(heads == head, map_lambda[...], 0.0), axis=1, keepdims=True) for head in (0, 1)]
    lam = jnp.where(lane_first, lams[0], lams[1])
    difference = total[:PROP] - lam * total[PROP:]
    squared = difference * difference
    mean_first = jnp.sum(jnp.where(lane_first, squared, 0.0), axis=1, keepdims=True)
    mean_second = jnp.sum(jnp.where(lane_first, 0.0, squared), axis=1, keepdims=True)
    mean = jnp.where(lane_first, mean_first, mean_second) / HEAD
    normed = (difference * lax.rsqrt(mean + epsilon) * out_gain[pl.ds(pair, 1), :]).astype(bf16)
    for target in range(N_KV):
        copies[target] = normed


def output_kernel(arrived, w_output, copies):
    total = None
    for pair in range(PAIRS):
        rows = jnp.concatenate([arrived[seq * PAIRS + pair] for seq in range(SEQS)], axis=0)
        part = lax.dot_general(
            rows, w_output[pair * LANES : (pair + 1) * LANES, :], NN, preferred_element_type=f32
        )
        total = part if total is None else total + part
    total = total.astype(bf16)
    for target in range(N_TP):
        copies[target] = total


def mix_kernel(arrived, out):
    total = arrived[0].astype(f32)
    for source in range(1, N_TP):
        total = total + arrived[source].astype(f32)
    out[...] = total.astype(bf16)


def vmem():
    return pl.BlockSpec(memory_space=pltpu.VMEM)


def hbm():
    return pl.BlockSpec(memory_space=pltpu.HBM)


def smem():
    return pl.BlockSpec(memory_space=pltpu.SMEM)


def shape(dims, kind=bf16):
    return jax.ShapeDtypeStruct(dims, kind)


def room(mebibytes):
    return pltpu.CompilerParams(vmem_limit_bytes=mebibytes * 1024 * 1024)


def near(dims, kind=bf16):
    return pltpu.VMEM(dims, kind)


def far(*arrays):
    return [pltpu.with_memory_space_constraint(array, pltpu.HBM) for array in arrays]


def cost(flops, moved):
    return pl.CostEstimate(flops=flops, bytes_accessed=moved, transcendentals=0)


def local(
    tokens,
    norm_gain,
    w_query,
    w_key,
    w_value,
    w_output,
    cache_keys,
    cache_values,
    map_lambda,
    out_gain,
    parents,
    lengths,
    accepted,
):
    width = cache_keys.shape[2]
    exchange = functools.partial(lax.all_to_all, split_axis=0, concat_axis=0, tiled=True)

    partial = pl.pallas_call(
        project_kernel,
        out_shape=near((N_KV, 80, LANES)),
        in_specs=[hbm()] * 5,
        out_specs=vmem(),
        scratch_shapes=[
            pltpu.VMEM(tokens.shape, bf16),
            pltpu.VMEM((1, norm_gain.shape[0]), f32),
            pltpu.VMEM(w_query.shape, bf16),
            pltpu.VMEM(w_key.shape, bf16),
            pltpu.VMEM(w_value.shape, bf16),
            pltpu.SemaphoreType.DMA((5,)),
        ],
        compiler_params=room(8),
        cost_estimate=cost(20_000_000_000, 40_000_000),
        name="project",
    )(*far(tokens, norm_gain.reshape(1, -1), w_query, w_key, w_value))
    near_keys = pltpu.with_memory_space_constraint(cache_keys, pltpu.VMEM)
    near_values = pltpu.with_memory_space_constraint(cache_values, pltpu.VMEM)
    arrived = exchange(partial, "kv")
    own, copies = pl.pallas_call(
        normalize_kernel,
        out_shape=(near((72, LANES)), near((N_KV, 72, LANES))),
        in_specs=[vmem()],
        out_specs=(vmem(), vmem()),
        compiler_params=room(8),
        cost_estimate=cost(20_000_000_000, 40_000_000),
        name="normalize",
    )(arrived)
    gathered = exchange(copies, "kv")
    parts = pl.pallas_call(
        attend_kernel,
        out_shape=shape((N_KV, 56, LANES)),
        in_specs=[vmem()] * 5,
        out_specs=hbm(),
        scratch_shapes=[
            pltpu.VMEM((N_KV, 56, LANES), bf16),
            pltpu.SemaphoreType.DMA((SEQS,)),
        ],
        compiler_params=room(24),
        name="attend",
    )(lengths.reshape(1, -1), accepted.reshape(1, -1), gathered, near_keys, near_values)
    arrived_parts = exchange(parts, "kv")
    new_keys, new_values, own_part = pl.pallas_call(
        write_kernel,
        out_shape=(shape(cache_keys.shape), shape(cache_values.shape), near((96, LANES), f32)),
        in_specs=[smem(), smem()] + [vmem()] * 3 + [hbm(), hbm()],
        out_specs=(hbm(), hbm(), vmem()),
        scratch_shapes=[
            pltpu.VMEM(cache_keys.shape, bf16),
            pltpu.VMEM(cache_values.shape, bf16),
            pltpu.VMEM((SEQS, 2, WINDOW, width), bf16),
            pltpu.SemaphoreType.DMA((SEQS, 2)),
            pltpu.SemaphoreType.DMA((SEQS, 2)),
            pltpu.SemaphoreType.DMA((SEQS, 2)),
        ],
        compiler_params=room(24),
        cost_estimate=cost(8_000_000_000, 8_000_000),
        name="write",
    )(lengths, accepted, gathered, parents, own, *far(cache_keys, cache_values))
    normed = pl.pallas_call(
        finish_kernel,
        out_shape=near((N_KV, PROP, LANES)),
        in_specs=[vmem()] * 4,
        out_specs=vmem(),
        compiler_params=room(8),
        name="finish",
    )(map_lambda.reshape(1, -1), out_gain.reshape(PAIRS, LANES), arrived_parts, own_part)
    arrived_normed = exchange(normed, "kv")
    partial_out = pl.pallas_call(
        output_kernel,
        out_shape=near((N_TP, SEQS * PROP, w_output.shape[1])),
        in_specs=[vmem(), vmem()],
        out_specs=vmem(),
        compiler_params=room(8),
        name="output",
    )(arrived_normed, w_output)
    arrived_out = exchange(partial_out, "tp")
    mixed = pl.pallas_call(
        mix_kernel,
        out_shape=shape((SEQS * PROP, w_output.shape[1])),
        in_specs=[vmem()],
        out_specs=vmem(),
        compiler_params=room(8),
        name="mix",
    )(arrived_out)
    return (mixed, new_keys, new_values)


def solution(mesh):
    return jax.shard_map(
        local,
        mesh=mesh,
        in_specs=(
            P(None, "kv"),
            P("kv"),
            P("kv", "tp"),
            P("kv", "tp"),
            P("kv", "tp"),
            P("tp", "kv"),
            P(None, "kv", "tp"),
            P(None, "kv", "tp"),
            P("tp"),
            P("tp"),
            P(),
            P(),
            P(),
        ),
        out_specs=(P(None, "kv"), P(None, "kv", "tp"), P(None, "kv", "tp")),
        check_vma=False,
    )
```

```python
import functools

import jax
import jax.numpy as jnp
from jax import lax
from jax.experimental import pallas as pl
from jax.experimental.pallas import tpu as pltpu
from jax.sharding import PartitionSpec as P

D = 4096
HEAD = 64
QK = 32
SEQS = 4
PROP = 24
PAIRS = 4
LANES = 128
N_KV = 16
N_TP = 8
WINDOW = 48
LAG = 3
ROWS = 96
QUERY_ROWS = PAIRS * ROWS
PAIR_ROWS = PAIRS * PROP

f32 = jnp.float32
bf16 = jnp.bfloat16
epsilon = 1e-05
masked_low = -1e30
score_scale = QK ** (-0.5)
LOG2E = 1.4426950408889634

NT = (((1,), (1,)), ((), ()))
NN = (((1,), (0,)), ((), ()))


def iota(shape, dim):
    return lax.broadcasted_iota(jnp.int32, shape, dim)


def three_parts(first, second):
    place = iota((8, LANES), 0)
    wide = jnp.where(place % 2 == 0, first, second)
    high = wide.astype(bf16).astype(f32)
    rest = wide - high
    middle = rest.astype(bf16).astype(f32)
    low = rest - middle
    tile = jnp.where(place < 2, high, jnp.where(place < 4, middle, jnp.where(place < 6, low, 0.0)))
    return tile.astype(bf16)


def column_to_row(column):
    count = column.shape[0]
    eye = iota((count, LANES), 0) == iota((count, LANES), 1)
    return jnp.sum(jnp.where(eye, column, 0.0), axis=0, keepdims=True)


def row_to_column(row, count):
    eye = iota((count, LANES), 0) == iota((count, LANES), 1)
    return jnp.sum(jnp.where(eye, row, 0.0), axis=1, keepdims=True)


def project_kernel(tokens_far, gain_far, query_far, key_far, value_far, *refs):
    outs, (tokens, gain, query, key, value, rows, done) = refs[:4], refs[4:]
    far = (tokens_far, gain_far, query_far, key_far, value_far)
    near = (tokens, gain, query, key, value)
    loads = [pltpu.make_async_copy(a, b, done.at[place]) for place, (a, b) in enumerate(zip(far, near))]
    for load in loads:
        load.start()
    for load in loads[:2]:
        load.wait()
    wide = tokens[...].astype(f32)
    gained = (wide * gain[...]).astype(bf16)
    row = column_to_row(jnp.sum(wide * wide, axis=1, keepdims=True))
    tile = three_parts(row, row)
    mine = lax.axis_index("kv") // PAIRS
    for out in outs:
        out[QUERY_ROWS + 2 * PAIR_ROWS :, :] = tile
    for place, weight in enumerate((query, key, value)):
        loads[2 + place].wait()
        product = lax.dot_general(gained, weight[...], NN, preferred_element_type=f32)
        if place == 0:
            narrow = product.astype(bf16)
            for out in outs:
                for pair in range(PAIRS):
                    out[pair * ROWS : (pair + 1) * ROWS, :] = narrow[:, pair * LANES : (pair + 1) * LANES]
        else:
            rows[...] = product
            for step, out in enumerate(outs):
                begin = pl.multiple_of((mine + step) % SEQS * PROP, 8)
                part = rows[pl.ds(begin, PROP), :].astype(bf16)
                for pair in range(PAIRS):
                    start = QUERY_ROWS + (place - 1) * PAIR_ROWS + pair * PROP
                    out[start : start + PROP, :] = part[:, pair * LANES : (pair + 1) * LANES]


def summed_squares(arrays, start):
    tile = sum(array[start:, :].astype(f32) for array in arrays)
    return tile[0:1] + tile[2:3] + tile[4:5]


def fold_kernel(*refs):
    arrays, outs, pairs = refs[:4], refs[4:8], refs[8]
    for pair in range(PAIRS):
        rows = slice(pair * ROWS, (pair + 1) * ROWS)
        total = sum(array[rows, :].astype(f32) for array in arrays).astype(bf16)
        for out in outs:
            out[rows, :] = total
    row = summed_squares(arrays, QUERY_ROWS + 2 * PAIR_ROWS)
    tile = three_parts(row, row)
    pairs[...] = sum(array[QUERY_ROWS : QUERY_ROWS + 2 * PAIR_ROWS, :].astype(f32) for array in arrays)
    mine = lax.axis_index("kv") % PAIRS
    for step, out in enumerate(outs):
        for place in range(2):
            begin = pl.multiple_of((mine + step) % PAIRS * PROP + place * PAIR_ROWS, 8)
            start = QUERY_ROWS + place * PROP
            out[start : start + PROP, :] = pairs[pl.ds(begin, PROP), :].astype(bf16)
        out[QUERY_ROWS + 2 * PROP :, :] = tile


def normalize_kernel(first, second, third, fourth, queries, own):
    arrays = (first, second, third, fourth)
    factor = lax.rsqrt(row_to_column(summed_squares(arrays, QUERY_ROWS + 2 * PROP), ROWS) / D + epsilon)
    scaled = factor * (score_scale * LOG2E)
    for pair in range(PAIRS):
        rows = slice(pair * ROWS, (pair + 1) * ROWS)
        queries[rows, :] = (sum(array[rows, :].astype(f32) for array in arrays) * scaled).astype(bf16)
    mine = lax.axis_index("kv") // PAIRS
    chosen = factor[:PROP]
    for seq in range(1, SEQS):
        chosen = jnp.where(mine == seq, factor[seq * PROP : (seq + 1) * PROP], chosen)
    for place in range(2):
        rows = slice(QUERY_ROWS + place * PROP, QUERY_ROWS + (place + 1) * PROP)
        total = sum(array[rows, :].astype(f32) for array in arrays)
        own[place * PROP : (place + 1) * PROP, :] = (total * chosen).astype(bf16)


def expanded(queries):
    group = iota(queries.shape, 1) // QK
    zero = jnp.zeros_like(queries)
    return jnp.concatenate([jnp.where(group == place, queries, zero) for place in range(4)], axis=0)


def by_head(array):
    return jnp.where(iota((48, LANES), 1) < HEAD, array[:48], array[48:])


def own_steps(parents, all_queries, own, out):
    eye = iota((PROP, PROP), 0) == iota((PROP, PROP), 1)
    links = parents[pl.ds(lax.axis_index("kv") // PAIRS, 1), :].astype(f32)
    column = jnp.sum(jnp.where(eye, links, 0.0), axis=1, keepdims=True)
    reached = jnp.where(eye | (column == iota((PROP, PROP), 1).astype(f32)), 1.0, 0.0)
    device = lax.axis_index("kv")
    begin = (device % PAIRS) * ROWS + (device // PAIRS) * PROP
    queries = all_queries[pl.ds(pl.multiple_of(begin, 8), PROP), :]
    keys, values = own[:PROP, :], own[PROP:, :]
    scores = lax.dot_general(expanded(queries), keys, NT, preferred_element_type=f32)
    yield
    for _ in range(5):
        narrow = reached.astype(bf16)
        reached = jnp.minimum(1.0, lax.dot_general(narrow, narrow, NN, preferred_element_type=f32))
        yield
    related = jnp.concatenate([reached] * 4, axis=0) > 0.5
    scores = jnp.where(related, scores, masked_low)
    largest = jnp.max(scores, axis=1, keepdims=True)
    yield
    weight = jnp.where(related, jnp.exp2(scores - largest), 0.0)
    total = jnp.sum(weight, axis=1, keepdims=True)
    yield
    product = lax.dot_general(weight.astype(bf16), values, NN, preferred_element_type=f32)
    yield
    out[:48, :] = by_head(product / total)
    out[48:, :] = by_head(jnp.broadcast_to(largest + jnp.log2(total), (96, LANES)))
    yield


def attend_kernel(
    lengths,
    accepted,
    gathered,
    keys,
    values,
    out_far,
    out,
    sent,
):
    block_len = keys.shape[1]
    ends = lengths[...] + accepted[...] - lax.axis_index("kv") * block_len
    sends = [
        pltpu.make_async_copy(
            out.at[pl.ds(seq * PAIRS, PAIRS)], out_far.at[pl.ds(seq * PAIRS, PAIRS)], sent.at[seq]
        )
        for seq in range(SEQS)
    ]
    def scored(seq, pair):
        lanes = slice(pair * LANES, (pair + 1) * LANES)
        start = pair * ROWS + seq * PROP
        queries = expanded(gathered[start : start + PROP, :])
        return lax.dot_general(queries, keys[seq, :, lanes], NT, preferred_element_type=f32)

    def weighed(seq, scores):
        visible = iota((1, block_len), 1) < ends[:, seq : seq + 1]
        scores = jnp.where(visible, scores, masked_low)
        largest = jnp.max(scores, axis=1, keepdims=True)
        return largest, jnp.exp2(scores - largest).astype(bf16)

    ones = jnp.ones((block_len, LANES), bf16)
    eye = iota((48, LANES), 0) == iota((48, LANES), 1)

    def finished(seq, pair, largest, weight):
        lanes = slice(pair * LANES, (pair + 1) * LANES)
        both = jnp.concatenate([values[seq, :, lanes], ones], axis=1)
        product = lax.dot_general(weight, both, NN, preferred_element_type=f32)
        total = product[:, LANES:]
        out[seq * PAIRS + pair, :48, :] = by_head(product[:, :LANES] / total).astype(bf16)
        level = largest + jnp.log2(total)
        first = jnp.sum(jnp.where(eye, level[:48], 0.0), axis=0, keepdims=True)
        second = jnp.sum(jnp.where(eye, level[48:], 0.0), axis=0, keepdims=True)
        seen = ends[:, seq : seq + 1] > 0
        tile = three_parts(jnp.where(seen, first, masked_low), jnp.where(seen, second, masked_low))
        out[seq * PAIRS + pair, 48:, :] = tile

    units = [(seq, pair) for seq in range(SEQS) for pair in range(PAIRS)]
    scores = scored(*units[0])
    waiting = []
    for place in range(len(units) + LAG):
        if place < len(units):
            following = scored(*units[place + 1]) if place + 1 < len(units) else None
            waiting.append((units[place], weighed(units[place][0], scores)))
            scores = following
        if place >= LAG:
            (seq, pair), found = waiting.pop(0)
            finished(seq, pair, *found)
            if pair == PAIRS - 1:
                sends[seq].start()
    for send in sends:
        send.wait()


def write_kernel(
    queries, parents, own, keys_far, values_far, new_keys, new_values, own_part, keys, values, loaded, stored
):
    pieces = [
        (seq, place, source, middle, target)
        for seq in range(SEQS)
        for place, (source, middle, target) in enumerate(
            ((keys_far, keys, new_keys), (values_far, values, new_values))
        )
    ]
    loads = [pltpu.make_async_copy(a.at[seq], b.at[seq], loaded.at[seq, place]) for seq, place, a, b, _ in pieces]
    stores = [pltpu.make_async_copy(b.at[seq], c.at[seq], stored.at[seq, place]) for seq, place, _, b, c in pieces]
    for load in loads:
        load.start()
    for _ in own_steps(parents, queries, own, own_part):
        pass
    for load, store in zip(loads, stores):
        load.wait()
        store.start()
    for store in stores:
        store.wait()


def patch_kernel(lengths, accepted, gathered, keys, values, new_keys, new_values, window, loaded, stored):
    block_len = keys.shape[1]
    offset = lax.axis_index("kv") * block_len
    pieces = []
    for seq in range(SEQS):
        begin = lengths[seq] + accepted[seq] - offset
        base = pl.multiple_of(jnp.clip((begin // 16) * 16, 0, block_len - WINDOW), 16)
        here = (begin > -PROP) & (begin < block_len)
        spans = [
            (source.at[seq, pl.ds(base, WINDOW)], window.at[seq, place], target.at[seq, pl.ds(base, WINDOW)])
            for place, (source, target) in enumerate(((keys, new_keys), (values, new_values)))
        ]
        loads = [pltpu.make_async_copy(a, b, loaded.at[seq, place]) for place, (a, b, _) in enumerate(spans)]
        stores = [pltpu.make_async_copy(b, c, stored.at[seq, place]) for place, (_, b, c) in enumerate(spans)]
        pieces.append((base - begin, here, loads, stores))
    for _, here, loads, _ in pieces:

        @pl.when(here)
        def _():
            for load in loads:
                load.start()

    for seq, (shift, here, loads, stores) in enumerate(pieces):

        @pl.when(here)
        def _():
            placing = (shift + iota((WINDOW, PROP), 0) == iota((WINDOW, PROP), 1)).astype(bf16)
            row = shift + iota((WINDOW, PAIRS * LANES), 0)
            written = (row >= 0) & (row < PROP)
            for place in range(2):
                span = slice((place + 1) * PROP, (place + 2) * PROP)
                rows = jnp.concatenate([gathered[seq * PAIRS + pair, span, :] for pair in range(PAIRS)], axis=1)
                moved_rows = lax.dot_general(placing, rows, NN, preferred_element_type=f32)
                loads[place].wait()
                old = window[seq, place].astype(f32)
                window[seq, place] = jnp.where(written, moved_rows, old).astype(bf16)
                stores[place].start()

    for _, here, _, stores in pieces:

        @pl.when(here)
        def _():
            for store in stores:
                store.wait()


def finish_kernel(map_lambda, out_gain, arrived, own_part, own, copies):
    pair = lax.axis_index("kv") % PAIRS
    lane = iota((48, LANES), 1)
    levels = jnp.concatenate([arrived[source, 48:, :].astype(f32) for source in range(N_KV)], axis=0).T[:48]
    levels = levels + pltpu.roll(levels, LANES - 2, 1) + pltpu.roll(levels, LANES - 4, 1)
    own_level = own_part[48:, :]
    is_first, is_second = lane % 8 == 0, lane % 8 == 1
    top = [
        jnp.maximum(
            jnp.max(jnp.where(mine, levels, masked_low), axis=1, keepdims=True), own_level[:, spot : spot + 1]
        )
        for mine, spot in ((is_first, 0), (is_second, HEAD))
    ]
    weights = jnp.exp2(jnp.where(is_first, levels - top[0], jnp.where(is_second, levels - top[1], masked_low)))
    own_weight = jnp.exp2(own_level - jnp.where(lane < HEAD, top[0], top[1]))
    sums = [jnp.sum(jnp.where(mine, weights, 0.0), axis=1, keepdims=True) for mine in (is_first, is_second)]
    whole = jnp.where(lane < HEAD, sums[0], sums[1]) + own_weight
    total = own_weight * own_part[:48, :]
    spot = jnp.where(lane < HEAD, 0, 1)
    for source in range(N_KV):
        factor = jnp.take_along_axis(weights, spot + 8 * source, axis=1, mode="promise_in_bounds")
        total = total + factor * arrived[source, :48, :].astype(f32)
    total = total / whole
    lane_first = iota((PROP, LANES), 1) < HEAD
    heads = iota((1, 8), 1) - 2 * pair
    lams = [jnp.sum(jnp.where(heads == head, map_lambda[...], 0.0), axis=1, keepdims=True) for head in (0, 1)]
    lam = jnp.where(lane_first, lams[0], lams[1])
    difference = total[:PROP] - lam * total[PROP:]
    squared = difference * difference
    mean_first = jnp.sum(jnp.where(lane_first, squared, 0.0), axis=1, keepdims=True)
    mean_second = jnp.sum(jnp.where(lane_first, 0.0, squared), axis=1, keepdims=True)
    mean = jnp.where(lane_first, mean_first, mean_second) / HEAD
    normed = (difference * lax.rsqrt(mean + epsilon) * out_gain[pl.ds(pair, 1), :]).astype(bf16)
    for target in range(N_KV):
        copies[target, :PROP, :] = normed
        copies[target, PROP:, :] = own[...]


def output_kernel(arrived, w_output, out):
    total = None
    for pair in range(PAIRS):
        rows = jnp.concatenate([arrived[seq * PAIRS + pair, :PROP, :] for seq in range(SEQS)], axis=0)
        part = lax.dot_general(
            rows, w_output[pair * LANES : (pair + 1) * LANES, :], NN, preferred_element_type=f32
        )
        total = part if total is None else total + part
    out[...] = total.astype(bf16)


def mix_kernel(*refs):
    out = refs[-1]
    out[...] = sum(ref[...].astype(f32) for ref in refs[:-1]).astype(bf16)


def vmem():
    return pl.BlockSpec(memory_space=pltpu.VMEM)


def hbm():
    return pl.BlockSpec(memory_space=pltpu.HBM)


def smem():
    return pl.BlockSpec(memory_space=pltpu.SMEM)


def shape(dims, kind=bf16):
    return jax.ShapeDtypeStruct(dims, kind)


def room(mebibytes):
    return pltpu.CompilerParams(vmem_limit_bytes=mebibytes * 1024 * 1024)


def near(dims, kind=bf16):
    return pltpu.VMEM(dims, kind)


def far(*arrays):
    return [pltpu.with_memory_space_constraint(array, pltpu.HBM) for array in arrays]


def cost(flops, moved):
    return pl.CostEstimate(flops=flops, bytes_accessed=moved, transcendentals=0)


def moved(arrays, axis, stride):
    count, size = len(arrays), lax.axis_size(axis)

    def target(index, step):
        place = index // stride % count
        return index + ((place + step) % count - place) * stride

    return [arrays[0]] + [
        lax.ppermute(arrays[step], axis, [(index, target(index, step)) for index in range(size)])
        for step in range(1, count)
    ]


def mix(kind, *arrays):
    return pl.pallas_call(
        mix_kernel,
        out_shape=kind(arrays[0].shape),
        in_specs=[vmem()] * len(arrays),
        out_specs=vmem(),
        compiler_params=room(8),
        name="mix",
    )(*arrays)


def local(
    tokens,
    norm_gain,
    w_query,
    w_key,
    w_value,
    w_output,
    cache_keys,
    cache_values,
    map_lambda,
    out_gain,
    parents,
    lengths,
    accepted,
):
    width = cache_keys.shape[2]
    exchange = functools.partial(lax.all_to_all, split_axis=0, concat_axis=0, tiled=True)

    partials = pl.pallas_call(
        project_kernel,
        out_shape=(near((QUERY_ROWS + 2 * PAIR_ROWS + 8, LANES)),) * 4,
        in_specs=[hbm()] * 5,
        out_specs=(vmem(),) * 4,
        scratch_shapes=[
            pltpu.VMEM(tokens.shape, bf16),
            pltpu.VMEM((1, norm_gain.shape[0]), f32),
            pltpu.VMEM(w_query.shape, bf16),
            pltpu.VMEM(w_key.shape, bf16),
            pltpu.VMEM(w_value.shape, bf16),
            pltpu.VMEM((ROWS, width), f32),
            pltpu.SemaphoreType.DMA((5,)),
        ],
        compiler_params=room(8),
        cost_estimate=cost(20_000_000_000, 40_000_000),
        name="project",
    )(*far(tokens, norm_gain.reshape(1, -1), w_query, w_key, w_value))
    near_keys = pltpu.with_memory_space_constraint(cache_keys, pltpu.VMEM)
    near_values = pltpu.with_memory_space_constraint(cache_values, pltpu.VMEM)
    folded = pl.pallas_call(
        fold_kernel,
        out_shape=(near((QUERY_ROWS + 2 * PROP + 8, LANES)),) * 4,
        in_specs=[vmem()] * 4,
        out_specs=(vmem(),) * 4,
        scratch_shapes=[pltpu.VMEM((2 * PAIR_ROWS, LANES), f32)],
        compiler_params=room(8),
        cost_estimate=cost(20_000_000_000, 40_000_000),
        name="fold",
    )(*moved(partials, "kv", 4))
    queries, own = pl.pallas_call(
        normalize_kernel,
        out_shape=(near((QUERY_ROWS, LANES)), near((2 * PROP, LANES))),
        in_specs=[vmem()] * 4,
        out_specs=(vmem(), vmem()),
        compiler_params=room(8),
        name="normalize",
    )(*moved(folded, "kv", 1))
    parts = pl.pallas_call(
        attend_kernel,
        out_shape=shape((N_KV, 56, LANES)),
        in_specs=[vmem()] * 5,
        out_specs=hbm(),
        scratch_shapes=[
            pltpu.VMEM((N_KV, 56, LANES), bf16),
            pltpu.SemaphoreType.DMA((SEQS,)),
        ],
        compiler_params=room(24),
        name="attend",
    )(lengths.reshape(1, -1), accepted.reshape(1, -1), queries, near_keys, near_values)
    arrived_parts = exchange(parts, "kv")
    copied_keys, copied_values, own_part = pl.pallas_call(
        write_kernel,
        out_shape=(shape(cache_keys.shape), shape(cache_values.shape), near((96, LANES), f32)),
        in_specs=[vmem()] * 3 + [hbm(), hbm()],
        out_specs=(hbm(), hbm(), vmem()),
        scratch_shapes=[
            pltpu.VMEM(cache_keys.shape, bf16),
            pltpu.VMEM(cache_values.shape, bf16),
            pltpu.SemaphoreType.DMA((SEQS, 2)),
            pltpu.SemaphoreType.DMA((SEQS, 2)),
        ],
        compiler_params=room(24),
        cost_estimate=cost(8_000_000_000, 8_000_000),
        name="write",
    )(queries, parents, own, *far(cache_keys, cache_values))
    normed = pl.pallas_call(
        finish_kernel,
        out_shape=near((N_KV, 3 * PROP, LANES)),
        in_specs=[vmem()] * 5,
        out_specs=vmem(),
        compiler_params=room(8),
        name="finish",
    )(map_lambda.reshape(1, -1), out_gain.reshape(PAIRS, LANES), arrived_parts, own_part, own)
    arrived_normed = exchange(normed, "kv")
    partial_out = pl.pallas_call(
        output_kernel,
        out_shape=near((ROWS, w_output.shape[1])),
        in_specs=[vmem(), vmem()],
        out_specs=vmem(),
        compiler_params=room(8),
        name="output",
    )(arrived_normed, w_output)
    paired = mix(near, *moved([partial_out] * 2, "tp", 1))
    new_keys, new_values = pl.pallas_call(
        patch_kernel,
        out_shape=(shape(cache_keys.shape), shape(cache_values.shape)),
        in_specs=[smem(), smem(), vmem(), hbm(), hbm()],
        out_specs=(hbm(), hbm()),
        scratch_shapes=[
            pltpu.VMEM((SEQS, 2, WINDOW, width), bf16),
            pltpu.SemaphoreType.DMA((SEQS, 2)),
            pltpu.SemaphoreType.DMA((SEQS, 2)),
        ],
        input_output_aliases={3: 0, 4: 1},
        compiler_params=room(8),
        cost_estimate=cost(4_000_000_000, 1_000_000),
        name="patch",
    )(lengths, accepted, arrived_normed, copied_keys, copied_values)
    mixed = mix(shape, *moved([paired] * 4, "tp", 2))
    return (mixed, new_keys, new_values)


def solution(mesh):
    return jax.shard_map(
        local,
        mesh=mesh,
        in_specs=(
            P(None, "kv"),
            P("kv"),
            P("kv", "tp"),
            P("kv", "tp"),
            P("kv", "tp"),
            P("tp", "kv"),
            P(None, "kv", "tp"),
            P(None, "kv", "tp"),
            P("tp"),
            P("tp"),
            P(),
            P(),
            P(),
        ),
        out_specs=(P(None, "kv"), P(None, "kv", "tp"), P(None, "kv", "tp")),
        check_vma=False,
    )
```

```python
import functools

import jax
import jax.numpy as jnp
from jax import lax
from jax.experimental import pallas as pl
from jax.experimental.pallas import tpu as pltpu
from jax.sharding import PartitionSpec as P

D = 4096
HEAD = 64
QK = 32
SEQS = 4
PROP = 24
PAIRS = 4
LANES = 128
N_KV = 16
N_TP = 8
WINDOW = 48
LAG = 3
ROWS = 96
QUERY_ROWS = PAIRS * ROWS
PAIR_ROWS = PAIRS * PROP

f32 = jnp.float32
bf16 = jnp.bfloat16
epsilon = 1e-05
masked_low = -1e30
score_scale = QK ** (-0.5)
LOG2E = 1.4426950408889634

NT = (((1,), (1,)), ((), ()))
NN = (((1,), (0,)), ((), ()))


def iota(shape, dim):
    return lax.broadcasted_iota(jnp.int32, shape, dim)


def three_parts(first, second):
    place = iota((8, LANES), 0)
    wide = jnp.where(place % 2 == 0, first, second)
    high = wide.astype(bf16).astype(f32)
    rest = wide - high
    middle = rest.astype(bf16).astype(f32)
    low = rest - middle
    tile = jnp.where(place < 2, high, jnp.where(place < 4, middle, jnp.where(place < 6, low, 0.0)))
    return tile.astype(bf16)


def column_to_row(column):
    count = column.shape[0]
    eye = iota((count, LANES), 0) == iota((count, LANES), 1)
    return jnp.sum(jnp.where(eye, column, 0.0), axis=0, keepdims=True)


def row_to_column(row, count):
    eye = iota((count, LANES), 0) == iota((count, LANES), 1)
    return jnp.sum(jnp.where(eye, row, 0.0), axis=1, keepdims=True)


def project_kernel(tokens_far, gain_far, query_far, key_far, value_far, *refs):
    outs, (tokens, gain, query, key, value, rows, done) = refs[:4], refs[4:]
    far = (tokens_far, gain_far, query_far, key_far, value_far)
    near = (tokens, gain, query, key, value)
    loads = [pltpu.make_async_copy(a, b, done.at[place]) for place, (a, b) in enumerate(zip(far, near))]
    for load in loads:
        load.start()
    for load in loads[:2]:
        load.wait()
    wide = tokens[...].astype(f32)
    gained = (wide * gain[...]).astype(bf16)
    row = column_to_row(jnp.sum(wide * wide, axis=1, keepdims=True))
    tile = three_parts(row, row)
    mine = lax.axis_index("kv") // PAIRS
    for out in outs:
        out[QUERY_ROWS + 2 * PAIR_ROWS :, :] = tile
    for place, weight in enumerate((query, key, value)):
        loads[2 + place].wait()
        product = lax.dot_general(gained, weight[...], NN, preferred_element_type=f32)
        if place == 0:
            narrow = product.astype(bf16)
            for out in outs:
                for pair in range(PAIRS):
                    out[pair * ROWS : (pair + 1) * ROWS, :] = narrow[:, pair * LANES : (pair + 1) * LANES]
        else:
            rows[...] = product
            for step, out in enumerate(outs):
                begin = pl.multiple_of((mine + step) % SEQS * PROP, 8)
                part = rows[pl.ds(begin, PROP), :].astype(bf16)
                for pair in range(PAIRS):
                    start = QUERY_ROWS + (place - 1) * PAIR_ROWS + pair * PROP
                    out[start : start + PROP, :] = part[:, pair * LANES : (pair + 1) * LANES]


def summed_squares(arrays, start):
    tile = sum(array[start:, :].astype(f32) for array in arrays)
    return tile[0:1] + tile[2:3] + tile[4:5]


def fold_kernel(*refs):
    arrays, outs, pairs = refs[:4], refs[4:8], refs[8]
    for pair in range(PAIRS):
        rows = slice(pair * ROWS, (pair + 1) * ROWS)
        total = sum(array[rows, :].astype(f32) for array in arrays).astype(bf16)
        for out in outs:
            out[rows, :] = total
    row = summed_squares(arrays, QUERY_ROWS + 2 * PAIR_ROWS)
    tile = three_parts(row, row)
    pairs[...] = sum(array[QUERY_ROWS : QUERY_ROWS + 2 * PAIR_ROWS, :].astype(f32) for array in arrays)
    mine = lax.axis_index("kv") % PAIRS
    for step, out in enumerate(outs):
        for place in range(2):
            begin = pl.multiple_of((mine + step) % PAIRS * PROP + place * PAIR_ROWS, 8)
            start = QUERY_ROWS + place * PROP
            out[start : start + PROP, :] = pairs[pl.ds(begin, PROP), :].astype(bf16)
        out[QUERY_ROWS + 2 * PROP :, :] = tile


def normalize_kernel(first, second, third, fourth, queries, own):
    arrays = (first, second, third, fourth)
    factor = lax.rsqrt(row_to_column(summed_squares(arrays, QUERY_ROWS + 2 * PROP), ROWS) / D + epsilon)
    scaled = factor * (score_scale * LOG2E)
    for pair in range(PAIRS):
        rows = slice(pair * ROWS, (pair + 1) * ROWS)
        queries[rows, :] = (sum(array[rows, :].astype(f32) for array in arrays) * scaled).astype(bf16)
    mine = lax.axis_index("kv") // PAIRS
    chosen = factor[:PROP]
    for seq in range(1, SEQS):
        chosen = jnp.where(mine == seq, factor[seq * PROP : (seq + 1) * PROP], chosen)
    for place in range(2):
        rows = slice(QUERY_ROWS + place * PROP, QUERY_ROWS + (place + 1) * PROP)
        total = sum(array[rows, :].astype(f32) for array in arrays)
        own[place * PROP : (place + 1) * PROP, :] = (total * chosen).astype(bf16)


def expanded(queries):
    group = iota(queries.shape, 1) // QK
    zero = jnp.zeros_like(queries)
    return jnp.concatenate([jnp.where(group == place, queries, zero) for place in range(4)], axis=0)


def by_head(array):
    return jnp.where(iota((48, LANES), 1) < HEAD, array[:48], array[48:])


def closure(parents):
    eye = iota((PROP, PROP), 0) == iota((PROP, PROP), 1)
    links = parents[pl.ds(lax.axis_index("kv") // PAIRS, 1), :].astype(f32)
    column = jnp.sum(jnp.where(eye, links, 0.0), axis=1, keepdims=True)
    reached = jnp.where(eye | (column == iota((PROP, PROP), 1).astype(f32)), 1.0, 0.0)
    for _ in range(5):
        narrow = reached.astype(bf16)
        reached = jnp.minimum(1.0, lax.dot_general(narrow, narrow, NN, preferred_element_type=f32))
    return reached


def own_steps(lineage, all_queries, own, out):
    device = lax.axis_index("kv")
    begin = (device % PAIRS) * ROWS + (device // PAIRS) * PROP
    queries = all_queries[pl.ds(pl.multiple_of(begin, 8), PROP), :]
    keys, values = own[:PROP, :], own[PROP:, :]
    scores = lax.dot_general(expanded(queries), keys, NT, preferred_element_type=f32)
    yield
    related = jnp.concatenate([lineage[...]] * 4, axis=0) > 0.5
    scores = jnp.where(related, scores, masked_low)
    largest = jnp.max(scores, axis=1, keepdims=True)
    yield
    weight = jnp.where(related, jnp.exp2(scores - largest), 0.0)
    total = jnp.sum(weight, axis=1, keepdims=True)
    yield
    product = lax.dot_general(weight.astype(bf16), values, NN, preferred_element_type=f32)
    yield
    out[:48, :] = by_head(product / total)
    out[48:, :] = by_head(jnp.broadcast_to(largest + jnp.log2(total), (96, LANES)))
    yield


def attend_kernel(lengths, accepted, gathered, keys, values, lineage, own, out, own_part):
    block_len = keys.shape[1]
    ends = lengths[...] + accepted[...] - lax.axis_index("kv") * block_len

    def scored(seq, pair):
        lanes = slice(pair * LANES, (pair + 1) * LANES)
        start = pair * ROWS + seq * PROP
        queries = expanded(gathered[start : start + PROP, :])
        return lax.dot_general(queries, keys[seq, :, lanes], NT, preferred_element_type=f32)

    def weighed(seq, scores):
        visible = iota((1, block_len), 1) < ends[:, seq : seq + 1]
        scores = jnp.where(visible, scores, masked_low)
        largest = jnp.max(scores, axis=1, keepdims=True)
        return largest, jnp.exp2(scores - largest).astype(bf16)

    ones = jnp.ones((block_len, LANES), bf16)
    eye = iota((48, LANES), 0) == iota((48, LANES), 1)

    def finished(seq, pair, largest, weight):
        lanes = slice(pair * LANES, (pair + 1) * LANES)
        both = jnp.concatenate([values[seq, :, lanes], ones], axis=1)
        product = lax.dot_general(weight, both, NN, preferred_element_type=f32)
        total = product[:, LANES:]
        out[seq * PAIRS + pair, :48, :] = by_head(product[:, :LANES] / total).astype(bf16)
        level = largest + jnp.log2(total)
        first = jnp.sum(jnp.where(eye, level[:48], 0.0), axis=0, keepdims=True)
        second = jnp.sum(jnp.where(eye, level[48:], 0.0), axis=0, keepdims=True)
        seen = ends[:, seq : seq + 1] > 0
        tile = three_parts(jnp.where(seen, first, masked_low), jnp.where(seen, second, masked_low))
        out[seq * PAIRS + pair, 48:, :] = tile

    units = [(seq, pair) for seq in range(SEQS) for pair in range(PAIRS)]
    steps = own_steps(lineage, gathered, own, own_part)
    scores = scored(*units[0])
    waiting = []
    for place in range(len(units) + LAG):
        if place < len(units):
            following = scored(*units[place + 1]) if place + 1 < len(units) else None
            waiting.append((units[place], weighed(units[place][0], scores)))
            scores = following
        if place >= LAG:
            (seq, pair), found = waiting.pop(0)
            finished(seq, pair, *found)
        if place >= 4:
            next(steps, None)


def copy_kernel(parents, keys_far, values_far, new_keys, new_values, keys, values, lineage, loaded, stored):
    pieces = [
        (seq, place, source, middle, target)
        for seq in range(SEQS)
        for place, (source, middle, target) in enumerate(
            ((keys_far, keys, new_keys), (values_far, values, new_values))
        )
    ]
    loads = [pltpu.make_async_copy(a.at[seq], b.at[seq], loaded.at[seq, place]) for seq, place, a, b, _ in pieces]
    stores = [pltpu.make_async_copy(b.at[seq], c.at[seq], stored.at[seq, place]) for seq, place, _, b, c in pieces]
    for load in loads:
        load.start()
    lineage[...] = closure(parents)
    for load, store in zip(loads, stores):
        load.wait()
        store.start()
    for store in stores:
        store.wait()


def patch_kernel(lengths, accepted, gathered, keys, values, new_keys, new_values, window, loaded, stored):
    block_len = keys.shape[1]
    offset = lax.axis_index("kv") * block_len
    pieces = []
    for seq in range(SEQS):
        begin = lengths[seq] + accepted[seq] - offset
        base = pl.multiple_of(jnp.clip((begin // 16) * 16, 0, block_len - WINDOW), 16)
        here = (begin > -PROP) & (begin < block_len)
        spans = [
            (source.at[seq, pl.ds(base, WINDOW)], window.at[seq, place], target.at[seq, pl.ds(base, WINDOW)])
            for place, (source, target) in enumerate(((keys, new_keys), (values, new_values)))
        ]
        loads = [pltpu.make_async_copy(a, b, loaded.at[seq, place]) for place, (a, b, _) in enumerate(spans)]
        stores = [pltpu.make_async_copy(b, c, stored.at[seq, place]) for place, (_, b, c) in enumerate(spans)]
        pieces.append((base - begin, here, loads, stores))
    for _, here, loads, _ in pieces:

        @pl.when(here)
        def _():
            for load in loads:
                load.start()

    for seq, (shift, here, loads, stores) in enumerate(pieces):

        @pl.when(here)
        def _():
            placing = (shift + iota((WINDOW, PROP), 0) == iota((WINDOW, PROP), 1)).astype(bf16)
            row = shift + iota((WINDOW, PAIRS * LANES), 0)
            written = (row >= 0) & (row < PROP)
            for place in range(2):
                span = slice((place + 1) * PROP, (place + 2) * PROP)
                rows = jnp.concatenate([gathered[seq * PAIRS + pair, span, :] for pair in range(PAIRS)], axis=1)
                moved_rows = lax.dot_general(placing, rows, NN, preferred_element_type=f32)
                loads[place].wait()
                old = window[seq, place].astype(f32)
                window[seq, place] = jnp.where(written, moved_rows, old).astype(bf16)
                stores[place].start()

    for _, here, _, stores in pieces:

        @pl.when(here)
        def _():
            for store in stores:
                store.wait()


def finish_kernel(map_lambda, out_gain, arrived, own_part, own, copies):
    pair = lax.axis_index("kv") % PAIRS
    lane = iota((48, LANES), 1)
    stacked = jnp.concatenate([arrived[source, 48:, :] for source in range(N_KV)], axis=0)
    eye = (iota((48, LANES), 0) == lane).astype(bf16)
    levels = lax.dot_general(eye, stacked, NT, preferred_element_type=f32)
    levels = levels + pltpu.roll(levels, LANES - 2, 1) + pltpu.roll(levels, LANES - 4, 1)
    own_level = own_part[48:, :]
    is_first, is_second = lane % 8 == 0, lane % 8 == 1
    top = [
        jnp.maximum(
            jnp.max(jnp.where(mine, levels, masked_low), axis=1, keepdims=True), own_level[:, spot : spot + 1]
        )
        for mine, spot in ((is_first, 0), (is_second, HEAD))
    ]
    weights = jnp.exp2(jnp.where(is_first, levels - top[0], jnp.where(is_second, levels - top[1], masked_low)))
    own_weight = jnp.exp2(own_level - jnp.where(lane < HEAD, top[0], top[1]))
    sums = [jnp.sum(jnp.where(mine, weights, 0.0), axis=1, keepdims=True) for mine in (is_first, is_second)]
    whole = jnp.where(lane < HEAD, sums[0], sums[1]) + own_weight
    total = own_weight * own_part[:48, :]
    spot = jnp.where(lane < HEAD, 0, 1)
    for source in range(N_KV):
        factor = jnp.take_along_axis(weights, spot + 8 * source, axis=1, mode="promise_in_bounds")
        total = total + factor * arrived[source, :48, :].astype(f32)
    total = total / whole
    lane_first = iota((PROP, LANES), 1) < HEAD
    heads = iota((1, 8), 1) - 2 * pair
    lams = [jnp.sum(jnp.where(heads == head, map_lambda[...], 0.0), axis=1, keepdims=True) for head in (0, 1)]
    lam = jnp.where(lane_first, lams[0], lams[1])
    difference = total[:PROP] - lam * total[PROP:]
    squared = difference * difference
    mean_first = jnp.sum(jnp.where(lane_first, squared, 0.0), axis=1, keepdims=True)
    mean_second = jnp.sum(jnp.where(lane_first, 0.0, squared), axis=1, keepdims=True)
    mean = jnp.where(lane_first, mean_first, mean_second) / HEAD
    normed = (difference * lax.rsqrt(mean + epsilon) * out_gain[pl.ds(pair, 1), :]).astype(bf16)
    for target in range(N_KV):
        copies[target, :PROP, :] = normed
        copies[target, PROP:, :] = own[...]


def output_kernel(arrived, w_output, out):
    total = None
    for pair in range(PAIRS):
        rows = jnp.concatenate([arrived[seq * PAIRS + pair, :PROP, :] for seq in range(SEQS)], axis=0)
        part = lax.dot_general(
            rows, w_output[pair * LANES : (pair + 1) * LANES, :], NN, preferred_element_type=f32
        )
        total = part if total is None else total + part
    out[...] = total.astype(bf16)


def mix_kernel(*refs):
    out = refs[-1]
    out[...] = sum(ref[...].astype(f32) for ref in refs[:-1]).astype(bf16)


def vmem():
    return pl.BlockSpec(memory_space=pltpu.VMEM)


def hbm():
    return pl.BlockSpec(memory_space=pltpu.HBM)


def smem():
    return pl.BlockSpec(memory_space=pltpu.SMEM)


def shape(dims, kind=bf16):
    return jax.ShapeDtypeStruct(dims, kind)


def room(mebibytes):
    return pltpu.CompilerParams(vmem_limit_bytes=mebibytes * 1024 * 1024)


def near(dims, kind=bf16):
    return pltpu.VMEM(dims, kind)


def far(*arrays):
    return [pltpu.with_memory_space_constraint(array, pltpu.HBM) for array in arrays]


def cost(flops, moved):
    return pl.CostEstimate(flops=flops, bytes_accessed=moved, transcendentals=0)


def moved(arrays, axis, stride):
    count, size = len(arrays), lax.axis_size(axis)

    def target(index, step):
        place = index // stride % count
        return index + ((place + step) % count - place) * stride

    order = [step for step in (1, 3, 2) if step < count]
    arrived = [
        lax.ppermute(arrays[step], axis, [(index, target(index, step)) for index in range(size)])
        for step in order
    ]
    return [arrays[0]] + arrived


def mix(kind, *arrays):
    return pl.pallas_call(
        mix_kernel,
        out_shape=kind(arrays[0].shape),
        in_specs=[vmem()] * len(arrays),
        out_specs=vmem(),
        compiler_params=room(8),
        name="mix",
    )(*arrays)


def local(
    tokens,
    norm_gain,
    w_query,
    w_key,
    w_value,
    w_output,
    cache_keys,
    cache_values,
    map_lambda,
    out_gain,
    parents,
    lengths,
    accepted,
):
    width = cache_keys.shape[2]
    exchange = functools.partial(lax.all_to_all, split_axis=0, concat_axis=0, tiled=True)

    partials = pl.pallas_call(
        project_kernel,
        out_shape=(near((QUERY_ROWS + 2 * PAIR_ROWS + 8, LANES)),) * 4,
        in_specs=[hbm()] * 5,
        out_specs=(vmem(),) * 4,
        scratch_shapes=[
            pltpu.VMEM(tokens.shape, bf16),
            pltpu.VMEM((1, norm_gain.shape[0]), f32),
            pltpu.VMEM(w_query.shape, bf16),
            pltpu.VMEM(w_key.shape, bf16),
            pltpu.VMEM(w_value.shape, bf16),
            pltpu.VMEM((ROWS, width), f32),
            pltpu.SemaphoreType.DMA((5,)),
        ],
        compiler_params=room(8),
        cost_estimate=cost(20_000_000_000, 40_000_000),
        name="project",
    )(*far(tokens, norm_gain.reshape(1, -1), w_query, w_key, w_value))
    copied_keys, copied_values, near_keys, near_values, lineage = pl.pallas_call(
        copy_kernel,
        out_shape=(
            shape(cache_keys.shape),
            shape(cache_values.shape),
            near(cache_keys.shape),
            near(cache_values.shape),
            near((PROP, PROP), f32),
        ),
        in_specs=[vmem(), hbm(), hbm()],
        out_specs=(hbm(), hbm(), vmem(), vmem(), vmem()),
        scratch_shapes=[pltpu.SemaphoreType.DMA((SEQS, 2)), pltpu.SemaphoreType.DMA((SEQS, 2))],
        compiler_params=room(24),
        cost_estimate=cost(8_000_000_000, 8_000_000),
        name="copy",
    )(parents, *far(cache_keys, cache_values))
    folded = pl.pallas_call(
        fold_kernel,
        out_shape=(near((QUERY_ROWS + 2 * PROP + 8, LANES)),) * 4,
        in_specs=[vmem()] * 4,
        out_specs=(vmem(),) * 4,
        scratch_shapes=[pltpu.VMEM((2 * PAIR_ROWS, LANES), f32)],
        compiler_params=room(8),
        cost_estimate=cost(20_000_000_000, 40_000_000),
        name="fold",
    )(*moved(partials, "kv", 4))
    queries, own = pl.pallas_call(
        normalize_kernel,
        out_shape=(near((QUERY_ROWS, LANES)), near((2 * PROP, LANES))),
        in_specs=[vmem()] * 4,
        out_specs=(vmem(), vmem()),
        compiler_params=room(8),
        name="normalize",
    )(*moved(folded, "kv", 1))
    parts, own_part = pl.pallas_call(
        attend_kernel,
        out_shape=(near((N_KV, 56, LANES)), near((96, LANES), f32)),
        in_specs=[vmem()] * 7,
        out_specs=(vmem(), vmem()),
        compiler_params=room(24),
        name="attend",
    )(lengths.reshape(1, -1), accepted.reshape(1, -1), queries, near_keys, near_values, lineage, own)
    arrived_parts = exchange(parts, "kv")
    normed = pl.pallas_call(
        finish_kernel,
        out_shape=near((N_KV, 3 * PROP, LANES)),
        in_specs=[vmem()] * 5,
        out_specs=vmem(),
        compiler_params=room(8),
        name="finish",
    )(map_lambda.reshape(1, -1), out_gain.reshape(PAIRS, LANES), arrived_parts, own_part, own)
    arrived_normed = exchange(normed, "kv")
    partial_out = pl.pallas_call(
        output_kernel,
        out_shape=near((ROWS, w_output.shape[1])),
        in_specs=[vmem(), vmem()],
        out_specs=vmem(),
        compiler_params=room(8),
        name="output",
    )(arrived_normed, w_output)
    paired = mix(near, *moved([partial_out] * 2, "tp", 1))
    new_keys, new_values = pl.pallas_call(
        patch_kernel,
        out_shape=(shape(cache_keys.shape), shape(cache_values.shape)),
        in_specs=[smem(), smem(), vmem(), hbm(), hbm()],
        out_specs=(hbm(), hbm()),
        scratch_shapes=[
            pltpu.VMEM((SEQS, 2, WINDOW, width), bf16),
            pltpu.SemaphoreType.DMA((SEQS, 2)),
            pltpu.SemaphoreType.DMA((SEQS, 2)),
        ],
        input_output_aliases={3: 0, 4: 1},
        compiler_params=room(8),
        cost_estimate=cost(4_000_000_000, 1_000_000),
        name="patch",
    )(lengths, accepted, arrived_normed, copied_keys, copied_values)
    mixed = mix(shape, *moved([paired] * 4, "tp", 2))
    return (mixed, new_keys, new_values)


def solution(mesh):
    return jax.shard_map(
        local,
        mesh=mesh,
        in_specs=(
            P(None, "kv"),
            P("kv"),
            P("kv", "tp"),
            P("kv", "tp"),
            P("kv", "tp"),
            P("tp", "kv"),
            P(None, "kv", "tp"),
            P(None, "kv", "tp"),
            P("tp"),
            P("tp"),
            P(),
            P(),
            P(),
        ),
        out_specs=(P(None, "kv"), P(None, "kv", "tp"), P(None, "kv", "tp")),
        check_vma=False,
    )
```

```python
import functools

import jax
import jax.numpy as jnp
from jax import lax
from jax.experimental import pallas as pl
from jax.experimental.pallas import tpu as pltpu
from jax.sharding import PartitionSpec as P

D = 4096
HEAD = 64
QK = 32
SEQS = 4
PROP = 24
PAIRS = 4
LANES = 128
N_KV = 16
N_TP = 8
WINDOW = 48
LAG = 3
ROWS = 96
QUERY_ROWS = PAIRS * ROWS
PAIR_ROWS = PAIRS * PROP

f32 = jnp.float32
bf16 = jnp.bfloat16
epsilon = 1e-05
masked_low = -1e30
score_scale = QK ** (-0.5)
LOG2E = 1.4426950408889634

NT = (((1,), (1,)), ((), ()))
NN = (((1,), (0,)), ((), ()))


def iota(shape, dim):
    return lax.broadcasted_iota(jnp.int32, shape, dim)


def three_parts(first, second):
    place = iota((8, LANES), 0)
    wide = jnp.where(place % 2 == 0, first, second)
    high = wide.astype(bf16).astype(f32)
    rest = wide - high
    middle = rest.astype(bf16).astype(f32)
    low = rest - middle
    tile = jnp.where(place < 2, high, jnp.where(place < 4, middle, jnp.where(place < 6, low, 0.0)))
    return tile.astype(bf16)


def column_to_row(column):
    count = column.shape[0]
    eye = iota((count, LANES), 0) == iota((count, LANES), 1)
    return jnp.sum(jnp.where(eye, column, 0.0), axis=0, keepdims=True)


def row_to_column(row, count):
    eye = iota((count, LANES), 0) == iota((count, LANES), 1)
    return jnp.sum(jnp.where(eye, row, 0.0), axis=1, keepdims=True)


def project_kernel(tokens_far, gain_far, query_far, key_far, value_far, *refs):
    outs, (tokens, gain, query, key, value, rows, done) = refs[:4], refs[4:]
    far = (tokens_far, gain_far, query_far, key_far, value_far)
    near = (tokens, gain, query, key, value)
    loads = [pltpu.make_async_copy(a, b, done.at[place]) for place, (a, b) in enumerate(zip(far, near))]
    for load in loads:
        load.start()
    for load in loads[:2]:
        load.wait()
    wide = tokens[...].astype(f32)
    gained = (wide * gain[...]).astype(bf16)
    row = column_to_row(jnp.sum(wide * wide, axis=1, keepdims=True))
    tile = three_parts(row, row)
    mine = lax.axis_index("kv") // PAIRS
    for out in outs:
        out[QUERY_ROWS + 2 * PAIR_ROWS :, :] = tile
    for place, weight in enumerate((query, key, value)):
        loads[2 + place].wait()
        product = lax.dot_general(gained, weight[...], NN, preferred_element_type=f32)
        if place == 0:
            narrow = product.astype(bf16)
            for out in outs:
                for pair in range(PAIRS):
                    out[pair * ROWS : (pair + 1) * ROWS, :] = narrow[:, pair * LANES : (pair + 1) * LANES]
        else:
            rows[...] = product
            for step, out in enumerate(outs):
                begin = pl.multiple_of((mine + step) % SEQS * PROP, 8)
                part = rows[pl.ds(begin, PROP), :].astype(bf16)
                for pair in range(PAIRS):
                    start = QUERY_ROWS + (place - 1) * PAIR_ROWS + pair * PROP
                    out[start : start + PROP, :] = part[:, pair * LANES : (pair + 1) * LANES]


def summed_squares(arrays, start):
    tile = sum(array[start:, :].astype(f32) for array in arrays)
    return tile[0:1] + tile[2:3] + tile[4:5]


def fold_kernel(*refs):
    arrays, outs, pairs = refs[:4], refs[4:8], refs[8]
    for pair in range(PAIRS):
        rows = slice(pair * ROWS, (pair + 1) * ROWS)
        total = sum(array[rows, :].astype(f32) for array in arrays).astype(bf16)
        for out in outs:
            out[rows, :] = total
    row = summed_squares(arrays, QUERY_ROWS + 2 * PAIR_ROWS)
    tile = three_parts(row, row)
    pairs[...] = sum(array[QUERY_ROWS : QUERY_ROWS + 2 * PAIR_ROWS, :].astype(f32) for array in arrays)
    mine = lax.axis_index("kv") % PAIRS
    for step, out in enumerate(outs):
        for place in range(2):
            begin = pl.multiple_of((mine + step) % PAIRS * PROP + place * PAIR_ROWS, 8)
            start = QUERY_ROWS + place * PROP
            out[start : start + PROP, :] = pairs[pl.ds(begin, PROP), :].astype(bf16)
        out[QUERY_ROWS + 2 * PROP :, :] = tile


def normalize_kernel(first, second, third, fourth, queries, own):
    arrays = (first, second, third, fourth)
    factor = lax.rsqrt(row_to_column(summed_squares(arrays, QUERY_ROWS + 2 * PROP), ROWS) / D + epsilon)
    scaled = factor * (score_scale * LOG2E)
    for pair in range(PAIRS):
        rows = slice(pair * ROWS, (pair + 1) * ROWS)
        queries[rows, :] = (sum(array[rows, :].astype(f32) for array in arrays) * scaled).astype(bf16)
    mine = lax.axis_index("kv") // PAIRS
    chosen = factor[:PROP]
    for seq in range(1, SEQS):
        chosen = jnp.where(mine == seq, factor[seq * PROP : (seq + 1) * PROP], chosen)
    for place in range(2):
        rows = slice(QUERY_ROWS + place * PROP, QUERY_ROWS + (place + 1) * PROP)
        total = sum(array[rows, :].astype(f32) for array in arrays)
        own[place * PROP : (place + 1) * PROP, :] = (total * chosen).astype(bf16)


def expanded(queries):
    group = iota(queries.shape, 1) // QK
    zero = jnp.zeros_like(queries)
    return jnp.concatenate([jnp.where(group == place, queries, zero) for place in range(4)], axis=0)


def by_head(array):
    return jnp.where(iota((48, LANES), 1) < HEAD, array[:48], array[48:])


def closure(parents):
    eye = iota((PROP, PROP), 0) == iota((PROP, PROP), 1)
    links = parents[pl.ds(lax.axis_index("kv") // PAIRS, 1), :].astype(f32)
    column = jnp.sum(jnp.where(eye, links, 0.0), axis=1, keepdims=True)
    reached = jnp.where(eye | (column == iota((PROP, PROP), 1).astype(f32)), 1.0, 0.0)
    for _ in range(5):
        narrow = reached.astype(bf16)
        reached = jnp.minimum(1.0, lax.dot_general(narrow, narrow, NN, preferred_element_type=f32))
    return reached


def own_steps(lineage, all_queries, own, out):
    device = lax.axis_index("kv")
    begin = (device % PAIRS) * ROWS + (device // PAIRS) * PROP
    queries = all_queries[pl.ds(pl.multiple_of(begin, 8), PROP), :]
    keys, values = own[:PROP, :], own[PROP:, :]
    scores = lax.dot_general(expanded(queries), keys, NT, preferred_element_type=f32)
    yield
    related = jnp.concatenate([lineage[...]] * 4, axis=0) > 0.5
    scores = jnp.where(related, scores, masked_low)
    largest = jnp.max(scores, axis=1, keepdims=True)
    yield
    weight = jnp.where(related, jnp.exp2(scores - largest), 0.0)
    total = jnp.sum(weight, axis=1, keepdims=True)
    yield
    product = lax.dot_general(weight.astype(bf16), values, NN, preferred_element_type=f32)
    yield
    out[:48, :] = by_head(product / total)
    out[48:, :] = by_head(jnp.broadcast_to(largest + jnp.log2(total), (96, LANES)))
    yield


def attend_kernel(lengths, accepted, gathered, keys, values, lineage, own, out, own_part):
    block_len = keys.shape[1]
    ends = lengths[...] + accepted[...] - lax.axis_index("kv") * block_len

    def scored(seq, pair):
        lanes = slice(pair * LANES, (pair + 1) * LANES)
        start = pair * ROWS + seq * PROP
        queries = expanded(gathered[start : start + PROP, :])
        return lax.dot_general(queries, keys[seq, :, lanes], NT, preferred_element_type=f32)

    def weighed(seq, scores):
        visible = iota((1, block_len), 1) < ends[:, seq : seq + 1]
        scores = jnp.where(visible, scores, masked_low)
        largest = jnp.max(scores, axis=1, keepdims=True)
        return largest, jnp.exp2(scores - largest).astype(bf16)

    ones = jnp.ones((block_len, LANES), bf16)
    eye = iota((48, LANES), 0) == iota((48, LANES), 1)

    def finished(seq, pair, largest, weight):
        lanes = slice(pair * LANES, (pair + 1) * LANES)
        both = jnp.concatenate([values[seq, :, lanes], ones], axis=1)
        product = lax.dot_general(weight, both, NN, preferred_element_type=f32)
        total = product[:, LANES:]
        out[seq * PAIRS + pair, :48, :] = by_head(product[:, :LANES] / total).astype(bf16)
        level = largest + jnp.log2(total)
        first = jnp.sum(jnp.where(eye, level[:48], 0.0), axis=0, keepdims=True)
        second = jnp.sum(jnp.where(eye, level[48:], 0.0), axis=0, keepdims=True)
        seen = ends[:, seq : seq + 1] > 0
        tile = three_parts(jnp.where(seen, first, masked_low), jnp.where(seen, second, masked_low))
        out[seq * PAIRS + pair, 48:, :] = tile

    units = [(seq, pair) for seq in range(SEQS) for pair in range(PAIRS)]
    steps = own_steps(lineage, gathered, own, own_part)
    scores = scored(*units[0])
    waiting = []
    for place in range(len(units) + LAG):
        if place < len(units):
            following = scored(*units[place + 1]) if place + 1 < len(units) else None
            waiting.append((units[place], weighed(units[place][0], scores)))
            scores = following
        if place >= LAG:
            (seq, pair), found = waiting.pop(0)
            finished(seq, pair, *found)
        if place >= 4:
            next(steps, None)


def copy_kernel(parents, keys_far, values_far, new_keys, new_values, keys, values, lineage, loaded, stored):
    pieces = [
        (seq, place, source, middle, target)
        for seq in range(SEQS)
        for place, (source, middle, target) in enumerate(
            ((keys_far, keys, new_keys), (values_far, values, new_values))
        )
    ]
    loads = [pltpu.make_async_copy(a.at[seq], b.at[seq], loaded.at[seq, place]) for seq, place, a, b, _ in pieces]
    stores = [pltpu.make_async_copy(b.at[seq], c.at[seq], stored.at[seq, place]) for seq, place, _, b, c in pieces]
    for load in loads:
        load.start()
    lineage[...] = closure(parents)
    for load, store in zip(loads, stores):
        load.wait()
        store.start()
    for store in stores:
        store.wait()


def patch_kernel(lengths, accepted, gathered, keys, values, new_keys, new_values, window, loaded, stored):
    block_len = keys.shape[1]
    offset = lax.axis_index("kv") * block_len
    pieces = []
    for seq in range(SEQS):
        begin = lengths[seq] + accepted[seq] - offset
        base = pl.multiple_of(jnp.clip((begin // 16) * 16, 0, block_len - WINDOW), 16)
        here = (begin > -PROP) & (begin < block_len)
        spans = [
            (source.at[seq, pl.ds(base, WINDOW)], window.at[seq, place], target.at[seq, pl.ds(base, WINDOW)])
            for place, (source, target) in enumerate(((keys, new_keys), (values, new_values)))
        ]
        loads = [pltpu.make_async_copy(a, b, loaded.at[seq, place]) for place, (a, b, _) in enumerate(spans)]
        stores = [pltpu.make_async_copy(b, c, stored.at[seq, place]) for place, (_, b, c) in enumerate(spans)]
        pieces.append((base - begin, here, loads, stores))
    for _, here, loads, _ in pieces:

        @pl.when(here)
        def _():
            for load in loads:
                load.start()

    for seq, (shift, here, loads, stores) in enumerate(pieces):

        @pl.when(here)
        def _():
            placing = (shift + iota((WINDOW, PROP), 0) == iota((WINDOW, PROP), 1)).astype(bf16)
            row = shift + iota((WINDOW, PAIRS * LANES), 0)
            written = (row >= 0) & (row < PROP)
            for place in range(2):
                span = slice((place + 1) * PROP, (place + 2) * PROP)
                rows = jnp.concatenate([gathered[seq * PAIRS + pair, span, :] for pair in range(PAIRS)], axis=1)
                moved_rows = lax.dot_general(placing, rows, NN, preferred_element_type=f32)
                loads[place].wait()
                old = window[seq, place].astype(f32)
                window[seq, place] = jnp.where(written, moved_rows, old).astype(bf16)
                stores[place].start()

    for _, here, _, stores in pieces:

        @pl.when(here)
        def _():
            for store in stores:
                store.wait()


def finish_kernel(map_lambda, out_gain, arrived, own_part, own, copies):
    pair = lax.axis_index("kv") % PAIRS
    lane = iota((48, LANES), 1)
    stacked = jnp.concatenate([arrived[source, 48:, :] for source in range(N_KV)], axis=0)
    eye = (iota((48, LANES), 0) == lane).astype(bf16)
    levels = lax.dot_general(eye, stacked, NT, preferred_element_type=f32)
    levels = levels + pltpu.roll(levels, LANES - 2, 1) + pltpu.roll(levels, LANES - 4, 1)
    own_level = own_part[48:, :]
    is_first, is_second = lane % 8 == 0, lane % 8 == 1
    top = [
        jnp.maximum(
            jnp.max(jnp.where(mine, levels, masked_low), axis=1, keepdims=True), own_level[:, spot : spot + 1]
        )
        for mine, spot in ((is_first, 0), (is_second, HEAD))
    ]
    weights = jnp.exp2(jnp.where(is_first, levels - top[0], jnp.where(is_second, levels - top[1], masked_low)))
    own_weight = jnp.exp2(own_level - jnp.where(lane < HEAD, top[0], top[1]))
    sums = [jnp.sum(jnp.where(mine, weights, 0.0), axis=1, keepdims=True) for mine in (is_first, is_second)]
    whole = jnp.where(lane < HEAD, sums[0], sums[1]) + own_weight
    total = own_weight * own_part[:48, :]
    spot = jnp.where(lane < HEAD, 0, 1)
    for source in range(N_KV):
        factor = jnp.take_along_axis(weights, spot + 8 * source, axis=1, mode="promise_in_bounds")
        total = total + factor * arrived[source, :48, :].astype(f32)
    total = total / whole
    lane_first = iota((PROP, LANES), 1) < HEAD
    heads = iota((1, 8), 1) - 2 * pair
    lams = [jnp.sum(jnp.where(heads == head, map_lambda[...], 0.0), axis=1, keepdims=True) for head in (0, 1)]
    lam = jnp.where(lane_first, lams[0], lams[1])
    difference = total[:PROP] - lam * total[PROP:]
    squared = difference * difference
    mean_first = jnp.sum(jnp.where(lane_first, squared, 0.0), axis=1, keepdims=True)
    mean_second = jnp.sum(jnp.where(lane_first, 0.0, squared), axis=1, keepdims=True)
    mean = jnp.where(lane_first, mean_first, mean_second) / HEAD
    normed = (difference * lax.rsqrt(mean + epsilon) * out_gain[pl.ds(pair, 1), :]).astype(bf16)
    for target in range(N_KV):
        copies[target, :PROP, :] = normed
        copies[target, PROP:, :] = own[...]


def output_kernel(arrived, w_output, out):
    total = None
    for pair in range(PAIRS):
        rows = jnp.concatenate([arrived[seq * PAIRS + pair, :PROP, :] for seq in range(SEQS)], axis=0)
        part = lax.dot_general(
            rows, w_output[pair * LANES : (pair + 1) * LANES, :], NN, preferred_element_type=f32
        )
        total = part if total is None else total + part
    out[...] = total.astype(bf16)


def mix_kernel(*refs):
    out = refs[-1]
    out[...] = sum(ref[...].astype(f32) for ref in refs[:-1]).astype(bf16)


def vmem():
    return pl.BlockSpec(memory_space=pltpu.VMEM)


def hbm():
    return pl.BlockSpec(memory_space=pltpu.HBM)


def smem():
    return pl.BlockSpec(memory_space=pltpu.SMEM)


def shape(dims, kind=bf16):
    return jax.ShapeDtypeStruct(dims, kind)


def room(mebibytes):
    return pltpu.CompilerParams(vmem_limit_bytes=mebibytes * 1024 * 1024)


def near(dims, kind=bf16):
    return pltpu.VMEM(dims, kind)


def far(*arrays):
    return [pltpu.with_memory_space_constraint(array, pltpu.HBM) for array in arrays]


def cost(flops, moved):
    return pl.CostEstimate(flops=flops, bytes_accessed=moved, transcendentals=0)


def moved(arrays, axis, stride):
    count, size = len(arrays), lax.axis_size(axis)

    def target(index, step):
        place = index // stride % count
        return index + ((place + step) % count - place) * stride

    order = [step for step in ((1, 3, 2) if axis == 'kv' else (2, 3, 1)) if step < count]
    arrived = [
        lax.ppermute(arrays[step], axis, [(index, target(index, step)) for index in range(size)])
        for step in order
    ]
    return [arrays[0]] + arrived


def mix(kind, *arrays):
    return pl.pallas_call(
        mix_kernel,
        out_shape=kind(arrays[0].shape),
        in_specs=[vmem()] * len(arrays),
        out_specs=vmem(),
        compiler_params=room(8),
        name="mix",
    )(*arrays)


def local(
    tokens,
    norm_gain,
    w_query,
    w_key,
    w_value,
    w_output,
    cache_keys,
    cache_values,
    map_lambda,
    out_gain,
    parents,
    lengths,
    accepted,
):
    width = cache_keys.shape[2]
    exchange = functools.partial(lax.all_to_all, split_axis=0, concat_axis=0, tiled=True)

    partials = pl.pallas_call(
        project_kernel,
        out_shape=(near((QUERY_ROWS + 2 * PAIR_ROWS + 8, LANES)),) * 4,
        in_specs=[hbm()] * 5,
        out_specs=(vmem(),) * 4,
        scratch_shapes=[
            pltpu.VMEM(tokens.shape, bf16),
            pltpu.VMEM((1, norm_gain.shape[0]), f32),
            pltpu.VMEM(w_query.shape, bf16),
            pltpu.VMEM(w_key.shape, bf16),
            pltpu.VMEM(w_value.shape, bf16),
            pltpu.VMEM((ROWS, width), f32),
            pltpu.SemaphoreType.DMA((5,)),
        ],
        compiler_params=room(8),
        cost_estimate=cost(20_000_000_000, 40_000_000),
        name="project",
    )(*far(tokens, norm_gain.reshape(1, -1), w_query, w_key, w_value))
    copied_keys, copied_values, near_keys, near_values, lineage = pl.pallas_call(
        copy_kernel,
        out_shape=(
            shape(cache_keys.shape),
            shape(cache_values.shape),
            near(cache_keys.shape),
            near(cache_values.shape),
            near((PROP, PROP), f32),
        ),
        in_specs=[vmem(), hbm(), hbm()],
        out_specs=(hbm(), hbm(), vmem(), vmem(), vmem()),
        scratch_shapes=[pltpu.SemaphoreType.DMA((SEQS, 2)), pltpu.SemaphoreType.DMA((SEQS, 2))],
        compiler_params=room(24),
        cost_estimate=cost(8_000_000_000, 8_000_000),
        name="copy",
    )(parents, *far(cache_keys, cache_values))
    folded = pl.pallas_call(
        fold_kernel,
        out_shape=(near((QUERY_ROWS + 2 * PROP + 8, LANES)),) * 4,
        in_specs=[vmem()] * 4,
        out_specs=(vmem(),) * 4,
        scratch_shapes=[pltpu.VMEM((2 * PAIR_ROWS, LANES), f32)],
        compiler_params=room(8),
        cost_estimate=cost(20_000_000_000, 40_000_000),
        name="fold",
    )(*moved(partials, "kv", 4))
    queries, own = pl.pallas_call(
        normalize_kernel,
        out_shape=(near((QUERY_ROWS, LANES)), near((2 * PROP, LANES))),
        in_specs=[vmem()] * 4,
        out_specs=(vmem(), vmem()),
        compiler_params=room(8),
        name="normalize",
    )(*moved(folded, "kv", 1))
    parts, own_part = pl.pallas_call(
        attend_kernel,
        out_shape=(near((N_KV, 56, LANES)), near((96, LANES), f32)),
        in_specs=[vmem()] * 7,
        out_specs=(vmem(), vmem()),
        compiler_params=room(24),
        name="attend",
    )(lengths.reshape(1, -1), accepted.reshape(1, -1), queries, near_keys, near_values, lineage, own)
    arrived_parts = exchange(parts, "kv")
    normed = pl.pallas_call(
        finish_kernel,
        out_shape=near((N_KV, 3 * PROP, LANES)),
        in_specs=[vmem()] * 5,
        out_specs=vmem(),
        compiler_params=room(8),
        name="finish",
    )(map_lambda.reshape(1, -1), out_gain.reshape(PAIRS, LANES), arrived_parts, own_part, own)
    arrived_normed = exchange(normed, "kv")
    partial_out = pl.pallas_call(
        output_kernel,
        out_shape=near((ROWS, w_output.shape[1])),
        in_specs=[vmem(), vmem()],
        out_specs=vmem(),
        compiler_params=room(8),
        name="output",
    )(arrived_normed, w_output)
    paired = mix(near, *moved([partial_out] * 2, "tp", 1))
    new_keys, new_values = pl.pallas_call(
        patch_kernel,
        out_shape=(shape(cache_keys.shape), shape(cache_values.shape)),
        in_specs=[smem(), smem(), vmem(), hbm(), hbm()],
        out_specs=(hbm(), hbm()),
        scratch_shapes=[
            pltpu.VMEM((SEQS, 2, WINDOW, width), bf16),
            pltpu.SemaphoreType.DMA((SEQS, 2)),
            pltpu.SemaphoreType.DMA((SEQS, 2)),
        ],
        input_output_aliases={3: 0, 4: 1},
        compiler_params=room(8),
        cost_estimate=cost(4_000_000_000, 1_000_000),
        name="patch",
    )(lengths, accepted, arrived_normed, copied_keys, copied_values)
    mixed = mix(shape, *moved([paired] * 4, "tp", 2))
    return (mixed, new_keys, new_values)


def solution(mesh):
    return jax.shard_map(
        local,
        mesh=mesh,
        in_specs=(
            P(None, "kv"),
            P("kv"),
            P("kv", "tp"),
            P("kv", "tp"),
            P("kv", "tp"),
            P("tp", "kv"),
            P(None, "kv", "tp"),
            P(None, "kv", "tp"),
            P("tp"),
            P("tp"),
            P(),
            P(),
            P(),
        ),
        out_specs=(P(None, "kv"), P(None, "kv", "tp"), P(None, "kv", "tp")),
        check_vma=False,
    )
```

```python
import functools

import jax
import jax.numpy as jnp
from jax import lax
from jax.experimental import pallas as pl
from jax.experimental.pallas import tpu as pltpu
from jax.sharding import PartitionSpec as P

D = 4096
HEAD = 64
QK = 32
SEQS = 4
PROP = 24
PAIRS = 4
LANES = 128
N_KV = 16
N_TP = 8
WINDOW = 48
LAG = 3
ROWS = 96
QUERY_ROWS = PAIRS * ROWS
PAIR_ROWS = PAIRS * PROP

f32 = jnp.float32
bf16 = jnp.bfloat16
epsilon = 1e-05
masked_low = -1e30
score_scale = QK ** (-0.5)
LOG2E = 1.4426950408889634

NT = (((1,), (1,)), ((), ()))
NN = (((1,), (0,)), ((), ()))


def iota(shape, dim):
    return lax.broadcasted_iota(jnp.int32, shape, dim)


def three_parts(first, second):
    place = iota((8, LANES), 0)
    wide = jnp.where(place % 2 == 0, first, second)
    high = wide.astype(bf16).astype(f32)
    rest = wide - high
    middle = rest.astype(bf16).astype(f32)
    low = rest - middle
    tile = jnp.where(place < 2, high, jnp.where(place < 4, middle, jnp.where(place < 6, low, 0.0)))
    return tile.astype(bf16)


def column_to_row(column):
    count = column.shape[0]
    eye = iota((count, LANES), 0) == iota((count, LANES), 1)
    return jnp.sum(jnp.where(eye, column, 0.0), axis=0, keepdims=True)


def row_to_column(row, count):
    eye = iota((count, LANES), 0) == iota((count, LANES), 1)
    return jnp.sum(jnp.where(eye, row, 0.0), axis=1, keepdims=True)


def project_kernel(tokens_far, gain_far, query_far, key_far, value_far, *refs):
    outs, (tokens, gain, query, key, value, rows, done) = refs[:4], refs[4:]
    far = (tokens_far, gain_far, query_far, key_far, value_far)
    near = (tokens, gain, query, key, value)
    loads = [pltpu.make_async_copy(a, b, done.at[place]) for place, (a, b) in enumerate(zip(far, near))]
    for load in loads:
        load.start()
    for load in loads[:2]:
        load.wait()
    wide = tokens[...].astype(f32)
    gained = (wide * gain[...]).astype(bf16)
    row = column_to_row(jnp.sum(wide * wide, axis=1, keepdims=True))
    tile = three_parts(row, row)
    mine = lax.axis_index("kv") // PAIRS
    for out in outs:
        out[QUERY_ROWS + 2 * PAIR_ROWS :, :] = tile
    for place, weight in enumerate((query, key, value)):
        loads[2 + place].wait()
        product = lax.dot_general(gained, weight[...], NN, preferred_element_type=f32)
        if place == 0:
            narrow = product.astype(bf16)
            for out in outs:
                for pair in range(PAIRS):
                    out[pair * ROWS : (pair + 1) * ROWS, :] = narrow[:, pair * LANES : (pair + 1) * LANES]
        else:
            rows[...] = product
            for step, out in enumerate(outs):
                begin = pl.multiple_of((mine + step) % SEQS * PROP, 8)
                part = rows[pl.ds(begin, PROP), :].astype(bf16)
                for pair in range(PAIRS):
                    start = QUERY_ROWS + (place - 1) * PAIR_ROWS + pair * PROP
                    out[start : start + PROP, :] = part[:, pair * LANES : (pair + 1) * LANES]


def summed_squares(arrays, start):
    tile = sum(array[start:, :].astype(f32) for array in arrays)
    return tile[0:1] + tile[2:3] + tile[4:5]


def fold_kernel(*refs):
    arrays, outs, pairs = refs[:4], refs[5:9], refs[9]
    for pair in range(PAIRS):
        rows = slice(pair * ROWS, (pair + 1) * ROWS)
        total = sum(array[rows, :].astype(f32) for array in arrays).astype(bf16)
        for out in outs:
            out[rows, :] = total
    row = summed_squares(arrays, QUERY_ROWS + 2 * PAIR_ROWS)
    tile = three_parts(row, row)
    pairs[...] = sum(array[QUERY_ROWS : QUERY_ROWS + 2 * PAIR_ROWS, :].astype(f32) for array in arrays)
    mine = lax.axis_index("kv") % PAIRS
    for step, out in enumerate(outs):
        for place in range(2):
            begin = pl.multiple_of((mine + step) % PAIRS * PROP + place * PAIR_ROWS, 8)
            start = QUERY_ROWS + place * PROP
            out[start : start + PROP, :] = pairs[pl.ds(begin, PROP), :].astype(bf16)
        out[QUERY_ROWS + 2 * PROP :, :] = tile


def normalize_kernel(first, second, third, fourth, queries, own):
    arrays = (first, second, third, fourth)
    factor = lax.rsqrt(row_to_column(summed_squares(arrays, QUERY_ROWS + 2 * PROP), ROWS) / D + epsilon)
    scaled = factor * (score_scale * LOG2E)
    for pair in range(PAIRS):
        rows = slice(pair * ROWS, (pair + 1) * ROWS)
        queries[rows, :] = (sum(array[rows, :].astype(f32) for array in arrays) * scaled).astype(bf16)
    mine = lax.axis_index("kv") // PAIRS
    chosen = factor[:PROP]
    for seq in range(1, SEQS):
        chosen = jnp.where(mine == seq, factor[seq * PROP : (seq + 1) * PROP], chosen)
    for place in range(2):
        rows = slice(QUERY_ROWS + place * PROP, QUERY_ROWS + (place + 1) * PROP)
        total = sum(array[rows, :].astype(f32) for array in arrays)
        own[place * PROP : (place + 1) * PROP, :] = (total * chosen).astype(bf16)


def expanded(queries):
    group = iota(queries.shape, 1) // QK
    zero = jnp.zeros_like(queries)
    return jnp.concatenate([jnp.where(group == place, queries, zero) for place in range(4)], axis=0)


def by_head(array):
    return jnp.where(iota((48, LANES), 1) < HEAD, array[:48], array[48:])


def closure(parents):
    eye = iota((PROP, PROP), 0) == iota((PROP, PROP), 1)
    links = parents[pl.ds(lax.axis_index("kv") // PAIRS, 1), :].astype(f32)
    column = jnp.sum(jnp.where(eye, links, 0.0), axis=1, keepdims=True)
    reached = jnp.where(eye | (column == iota((PROP, PROP), 1).astype(f32)), 1.0, 0.0)
    for _ in range(5):
        narrow = reached.astype(bf16)
        reached = jnp.minimum(1.0, lax.dot_general(narrow, narrow, NN, preferred_element_type=f32))
    return reached


def own_steps(lineage, all_queries, own, out):
    device = lax.axis_index("kv")
    begin = (device % PAIRS) * ROWS + (device // PAIRS) * PROP
    queries = all_queries[pl.ds(pl.multiple_of(begin, 8), PROP), :]
    keys, values = own[:PROP, :], own[PROP:, :]
    scores = lax.dot_general(expanded(queries), keys, NT, preferred_element_type=f32)
    yield
    related = jnp.concatenate([lineage[...]] * 4, axis=0) > 0.5
    scores = jnp.where(related, scores, masked_low)
    largest = jnp.max(scores, axis=1, keepdims=True)
    yield
    weight = jnp.where(related, jnp.exp2(scores - largest), 0.0)
    total = jnp.sum(weight, axis=1, keepdims=True)
    yield
    product = lax.dot_general(weight.astype(bf16), values, NN, preferred_element_type=f32)
    yield
    out[:48, :] = by_head(product / total)
    out[48:, :] = by_head(jnp.broadcast_to(largest + jnp.log2(total), (96, LANES)))
    yield


def attend_kernel(lengths, accepted, gathered, keys, values, lineage, own, out, own_part):
    block_len = keys.shape[1]
    ends = lengths[...] + accepted[...] - lax.axis_index("kv") * block_len

    def scored(seq, pair):
        lanes = slice(pair * LANES, (pair + 1) * LANES)
        start = pair * ROWS + seq * PROP
        queries = expanded(gathered[start : start + PROP, :])
        return lax.dot_general(queries, keys[seq, :, lanes], NT, preferred_element_type=f32)

    def weighed(seq, scores):
        visible = iota((1, block_len), 1) < ends[:, seq : seq + 1]
        scores = jnp.where(visible, scores, masked_low)
        largest = jnp.max(scores, axis=1, keepdims=True)
        return largest, jnp.exp2(scores - largest).astype(bf16)

    ones = jnp.ones((block_len, LANES), bf16)
    eye = iota((48, LANES), 0) == iota((48, LANES), 1)

    def finished(seq, pair, largest, weight):
        lanes = slice(pair * LANES, (pair + 1) * LANES)
        both = jnp.concatenate([values[seq, :, lanes], ones], axis=1)
        product = lax.dot_general(weight, both, NN, preferred_element_type=f32)
        total = product[:, LANES:]
        out[seq * PAIRS + pair, :48, :] = by_head(product[:, :LANES] / total).astype(bf16)
        level = largest + jnp.log2(total)
        first = jnp.sum(jnp.where(eye, level[:48], 0.0), axis=0, keepdims=True)
        second = jnp.sum(jnp.where(eye, level[48:], 0.0), axis=0, keepdims=True)
        seen = ends[:, seq : seq + 1] > 0
        tile = three_parts(jnp.where(seen, first, masked_low), jnp.where(seen, second, masked_low))
        out[seq * PAIRS + pair, 48:, :] = tile

    units = [(seq, pair) for seq in range(SEQS) for pair in range(PAIRS)]
    steps = own_steps(lineage, gathered, own, own_part)
    scores = scored(*units[0])
    waiting = []
    for place in range(len(units) + LAG):
        if place < len(units):
            following = scored(*units[place + 1]) if place + 1 < len(units) else None
            waiting.append((units[place], weighed(units[place][0], scores)))
            scores = following
        if place >= LAG:
            (seq, pair), found = waiting.pop(0)
            finished(seq, pair, *found)
        if place >= 4:
            next(steps, None)


def copy_through(source, target, middle, loaded, stored, between=None):
    loads = [pltpu.make_async_copy(source.at[seq], middle.at[seq], loaded.at[seq]) for seq in range(SEQS)]
    stores = [pltpu.make_async_copy(middle.at[seq], target.at[seq], stored.at[seq]) for seq in range(SEQS)]
    for load in loads:
        load.start()
    if between is not None:
        between()
    for load, store in zip(loads, stores):
        load.wait()
        store.start()
    for store in stores:
        store.wait()


def copy_keys_kernel(parents, source, target, middle, lineage, loaded, stored):
    def between():
        lineage[...] = closure(parents)

    copy_through(source, target, middle, loaded, stored, between)


def copy_values_kernel(source, target, middle, loaded, stored):
    copy_through(source, target, middle, loaded, stored)


def patch_kernel(lengths, accepted, gathered, keys, values, new_keys, new_values, window, loaded, stored):
    block_len = keys.shape[1]
    offset = lax.axis_index("kv") * block_len
    pieces = []
    for seq in range(SEQS):
        begin = lengths[seq] + accepted[seq] - offset
        base = pl.multiple_of(jnp.clip((begin // 16) * 16, 0, block_len - WINDOW), 16)
        here = (begin > -PROP) & (begin < block_len)
        spans = [
            (source.at[seq, pl.ds(base, WINDOW)], window.at[seq, place], target.at[seq, pl.ds(base, WINDOW)])
            for place, (source, target) in enumerate(((keys, new_keys), (values, new_values)))
        ]
        loads = [pltpu.make_async_copy(a, b, loaded.at[seq, place]) for place, (a, b, _) in enumerate(spans)]
        stores = [pltpu.make_async_copy(b, c, stored.at[seq, place]) for place, (_, b, c) in enumerate(spans)]
        pieces.append((base - begin, here, loads, stores))
    for _, here, loads, _ in pieces:

        @pl.when(here)
        def _():
            for load in loads:
                load.start()

    for seq, (shift, here, loads, stores) in enumerate(pieces):

        @pl.when(here)
        def _():
            placing = (shift + iota((WINDOW, PROP), 0) == iota((WINDOW, PROP), 1)).astype(bf16)
            row = shift + iota((WINDOW, PAIRS * LANES), 0)
            written = (row >= 0) & (row < PROP)
            for place in range(2):
                span = slice((place + 1) * PROP, (place + 2) * PROP)
                rows = jnp.concatenate([gathered[seq * PAIRS + pair, span, :] for pair in range(PAIRS)], axis=1)
                moved_rows = lax.dot_general(placing, rows, NN, preferred_element_type=f32)
                loads[place].wait()
                old = window[seq, place].astype(f32)
                window[seq, place] = jnp.where(written, moved_rows, old).astype(bf16)
                stores[place].start()

    for _, here, _, stores in pieces:

        @pl.when(here)
        def _():
            for store in stores:
                store.wait()


def finish_kernel(map_lambda, out_gain, arrived, own_part, own, copies):
    pair = lax.axis_index("kv") % PAIRS
    lane = iota((48, LANES), 1)
    stacked = jnp.concatenate([arrived[source, 48:, :] for source in range(N_KV)], axis=0)
    eye = (iota((48, LANES), 0) == lane).astype(bf16)
    levels = lax.dot_general(eye, stacked, NT, preferred_element_type=f32)
    levels = levels + pltpu.roll(levels, LANES - 2, 1) + pltpu.roll(levels, LANES - 4, 1)
    own_level = own_part[48:, :]
    is_first, is_second = lane % 8 == 0, lane % 8 == 1
    top = [
        jnp.maximum(
            jnp.max(jnp.where(mine, levels, masked_low), axis=1, keepdims=True), own_level[:, spot : spot + 1]
        )
        for mine, spot in ((is_first, 0), (is_second, HEAD))
    ]
    weights = jnp.exp2(jnp.where(is_first, levels - top[0], jnp.where(is_second, levels - top[1], masked_low)))
    own_weight = jnp.exp2(own_level - jnp.where(lane < HEAD, top[0], top[1]))
    sums = [jnp.sum(jnp.where(mine, weights, 0.0), axis=1, keepdims=True) for mine in (is_first, is_second)]
    whole = jnp.where(lane < HEAD, sums[0], sums[1]) + own_weight
    total = own_weight * own_part[:48, :]
    spot = jnp.where(lane < HEAD, 0, 1)
    for source in range(N_KV):
        factor = jnp.take_along_axis(weights, spot + 8 * source, axis=1, mode="promise_in_bounds")
        total = total + factor * arrived[source, :48, :].astype(f32)
    total = total / whole
    lane_first = iota((PROP, LANES), 1) < HEAD
    heads = iota((1, 8), 1) - 2 * pair
    lams = [jnp.sum(jnp.where(heads == head, map_lambda[...], 0.0), axis=1, keepdims=True) for head in (0, 1)]
    lam = jnp.where(lane_first, lams[0], lams[1])
    difference = total[:PROP] - lam * total[PROP:]
    squared = difference * difference
    mean_first = jnp.sum(jnp.where(lane_first, squared, 0.0), axis=1, keepdims=True)
    mean_second = jnp.sum(jnp.where(lane_first, 0.0, squared), axis=1, keepdims=True)
    mean = jnp.where(lane_first, mean_first, mean_second) / HEAD
    normed = (difference * lax.rsqrt(mean + epsilon) * out_gain[pl.ds(pair, 1), :]).astype(bf16)
    for target in range(N_KV):
        copies[target, :PROP, :] = normed
        copies[target, PROP:, :] = own[...]


def output_kernel(arrived, w_output, out):
    total = None
    for pair in range(PAIRS):
        rows = jnp.concatenate([arrived[seq * PAIRS + pair, :PROP, :] for seq in range(SEQS)], axis=0)
        part = lax.dot_general(
            rows, w_output[pair * LANES : (pair + 1) * LANES, :], NN, preferred_element_type=f32
        )
        total = part if total is None else total + part
    out[...] = total.astype(bf16)


def mix_kernel(*refs):
    out = refs[-1]
    out[...] = sum(ref[...].astype(f32) for ref in refs[:-1]).astype(bf16)


def vmem():
    return pl.BlockSpec(memory_space=pltpu.VMEM)


def hbm():
    return pl.BlockSpec(memory_space=pltpu.HBM)


def smem():
    return pl.BlockSpec(memory_space=pltpu.SMEM)


def shape(dims, kind=bf16):
    return jax.ShapeDtypeStruct(dims, kind)


def room(mebibytes):
    return pltpu.CompilerParams(vmem_limit_bytes=mebibytes * 1024 * 1024)


def near(dims, kind=bf16):
    return pltpu.VMEM(dims, kind)


def far(*arrays):
    return [pltpu.with_memory_space_constraint(array, pltpu.HBM) for array in arrays]


def cost(flops, moved):
    return pl.CostEstimate(flops=flops, bytes_accessed=moved, transcendentals=0)


def moved(arrays, axis, stride):
    count, size = len(arrays), lax.axis_size(axis)

    def target(index, step):
        place = index // stride % count
        return index + ((place + step) % count - place) * stride

    order = [step for step in (1, 3, 2) if step < count]
    arrived = [
        lax.ppermute(arrays[step], axis, [(index, target(index, step)) for index in range(size)])
        for step in order
    ]
    return [arrays[0]] + arrived


def mix(kind, *arrays):
    return pl.pallas_call(
        mix_kernel,
        out_shape=kind(arrays[0].shape),
        in_specs=[vmem()] * len(arrays),
        out_specs=vmem(),
        compiler_params=room(8),
        name="mix",
    )(*arrays)


def local(
    tokens,
    norm_gain,
    w_query,
    w_key,
    w_value,
    w_output,
    cache_keys,
    cache_values,
    map_lambda,
    out_gain,
    parents,
    lengths,
    accepted,
):
    width = cache_keys.shape[2]
    exchange = functools.partial(lax.all_to_all, split_axis=0, concat_axis=0, tiled=True)

    partials = pl.pallas_call(
        project_kernel,
        out_shape=(near((QUERY_ROWS + 2 * PAIR_ROWS + 8, LANES)),) * 4,
        in_specs=[hbm()] * 5,
        out_specs=(vmem(),) * 4,
        scratch_shapes=[
            pltpu.VMEM(tokens.shape, bf16),
            pltpu.VMEM((1, norm_gain.shape[0]), f32),
            pltpu.VMEM(w_query.shape, bf16),
            pltpu.VMEM(w_key.shape, bf16),
            pltpu.VMEM(w_value.shape, bf16),
            pltpu.VMEM((ROWS, width), f32),
            pltpu.SemaphoreType.DMA((5,)),
        ],
        compiler_params=room(8),
        cost_estimate=cost(20_000_000_000, 40_000_000),
        name="project",
    )(*far(tokens, norm_gain.reshape(1, -1), w_query, w_key, w_value))
    copied_keys, near_keys, lineage = pl.pallas_call(
        copy_keys_kernel,
        out_shape=(shape(cache_keys.shape), near(cache_keys.shape), near((PROP, PROP), f32)),
        in_specs=[vmem(), hbm()],
        out_specs=(hbm(), vmem(), vmem()),
        scratch_shapes=[pltpu.SemaphoreType.DMA((SEQS,)), pltpu.SemaphoreType.DMA((SEQS,))],
        compiler_params=room(24),
        cost_estimate=cost(4_000_000_000, 4_000_000),
        name="copy_keys",
    )(parents, *far(cache_keys))
    copied_values, near_values = pl.pallas_call(
        copy_values_kernel,
        out_shape=(shape(cache_values.shape), near(cache_values.shape)),
        in_specs=[hbm()],
        out_specs=(hbm(), vmem()),
        scratch_shapes=[pltpu.SemaphoreType.DMA((SEQS,)), pltpu.SemaphoreType.DMA((SEQS,))],
        compiler_params=room(24),
        cost_estimate=cost(4_000_000_000, 4_000_000),
        name="copy_values",
    )(*far(cache_values))
    folded = pl.pallas_call(
        fold_kernel,
        out_shape=(near((QUERY_ROWS + 2 * PROP + 8, LANES)),) * 4,
        in_specs=[vmem()] * 5,
        out_specs=(vmem(),) * 4,
        scratch_shapes=[pltpu.VMEM((2 * PAIR_ROWS, LANES), f32)],
        compiler_params=room(8),
        cost_estimate=cost(20_000_000_000, 40_000_000),
        name="fold",
    )(*moved(partials, "kv", 4), lineage)
    queries, own = pl.pallas_call(
        normalize_kernel,
        out_shape=(near((QUERY_ROWS, LANES)), near((2 * PROP, LANES))),
        in_specs=[vmem()] * 4,
        out_specs=(vmem(), vmem()),
        compiler_params=room(8),
        name="normalize",
    )(*moved(folded, "kv", 1))
    parts, own_part = pl.pallas_call(
        attend_kernel,
        out_shape=(near((N_KV, 56, LANES)), near((96, LANES), f32)),
        in_specs=[vmem()] * 7,
        out_specs=(vmem(), vmem()),
        compiler_params=room(24),
        name="attend",
    )(lengths.reshape(1, -1), accepted.reshape(1, -1), queries, near_keys, near_values, lineage, own)
    arrived_parts = exchange(parts, "kv")
    normed = pl.pallas_call(
        finish_kernel,
        out_shape=near((N_KV, 3 * PROP, LANES)),
        in_specs=[vmem()] * 5,
        out_specs=vmem(),
        compiler_params=room(8),
        name="finish",
    )(map_lambda.reshape(1, -1), out_gain.reshape(PAIRS, LANES), arrived_parts, own_part, own)
    arrived_normed = exchange(normed, "kv")
    partial_out = pl.pallas_call(
        output_kernel,
        out_shape=near((ROWS, w_output.shape[1])),
        in_specs=[vmem(), vmem()],
        out_specs=vmem(),
        compiler_params=room(8),
        name="output",
    )(arrived_normed, w_output)
    paired = mix(near, *moved([partial_out] * 2, "tp", 1))
    new_keys, new_values = pl.pallas_call(
        patch_kernel,
        out_shape=(shape(cache_keys.shape), shape(cache_values.shape)),
        in_specs=[smem(), smem(), vmem(), hbm(), hbm()],
        out_specs=(hbm(), hbm()),
        scratch_shapes=[
            pltpu.VMEM((SEQS, 2, WINDOW, width), bf16),
            pltpu.SemaphoreType.DMA((SEQS, 2)),
            pltpu.SemaphoreType.DMA((SEQS, 2)),
        ],
        input_output_aliases={3: 0, 4: 1},
        compiler_params=room(8),
        cost_estimate=cost(4_000_000_000, 1_000_000),
        name="patch",
    )(lengths, accepted, arrived_normed, copied_keys, copied_values)
    mixed = mix(shape, *moved([paired] * 4, "tp", 2))
    return (mixed, new_keys, new_values)


def solution(mesh):
    return jax.shard_map(
        local,
        mesh=mesh,
        in_specs=(
            P(None, "kv"),
            P("kv"),
            P("kv", "tp"),
            P("kv", "tp"),
            P("kv", "tp"),
            P("tp", "kv"),
            P(None, "kv", "tp"),
            P(None, "kv", "tp"),
            P("tp"),
            P("tp"),
            P(),
            P(),
            P(),
        ),
        out_specs=(P(None, "kv"), P(None, "kv", "tp"), P(None, "kv", "tp")),
        check_vma=False,
    )
```
